256 devices in a mesh: ep: 64 (over z, x, core), tp: 4 (over y).
Axes of the slice: x: 4, y: 4, z: 8, core: 2. Of those that a mesh axis runs over, the one named last changes fastest.
Arguments:
- query_rows: bfloat16 [12288, 1024], P('ep', 'tp'), may hold values from -8 to 8
- key_rows: bfloat16 [12288, 1024], P('ep', 'tp'), may hold values from -8 to 8
- value_rows: bfloat16 [12288, 1024], P('ep', 'tp'), may hold values from -6 to 6
- lambdas: float32 [8], P('tp'), may hold values from 0.3 to 0.8
- head_gain: float32 [128], replicated, may hold values from 0.1 to 1.9
- w_out: bfloat16 [1024, 2048], replicated, may hold values from -0.1875 to 0.1875
- moe_rows: bfloat16 [32768, 2048], P('ep'), may hold values from -6 to 6
- ffn_gain: float32 [2048], replicated, may hold values from 0.1 to 1.9
- routes: int32 [32768, 2], P('ep'), may hold values from 0 to 63, all different within a row; in each aligned block of 128 rows (0 to 127, 128 to 255, ...) at most 8 rows name the same one
- group_logits: float32 [32768, 4], P('ep'), may hold values from -8 to 8
- pick_logits: float32 [32768, 2], P('ep'), may hold values from -8 to 8
- w_gate: bfloat16 [64, 2048, 1024], P('ep', None, 'tp'), may hold values from -0.125 to 0.125
- w_up: bfloat16 [64, 2048, 1024], P('ep', None, 'tp'), may hold values from -0.125 to 0.125
- w_down: bfloat16 [64, 1024, 2048], P('ep', 'tp'), may hold values from -0.75 to 0.75
Outputs:
- mixer_out: bfloat16 [12288, 2048], P(('ep', 'tp'))
- moe_out: bfloat16 [32768, 2048], P(('ep', 'tp'))
The draws below stay inside these ranges and needn't reach their ends.
Inputs may be any that keep to these rules, and one draw needn't show every extreme that they name: `routes`: each row names 2 different experts. In each aligned block of 128 rows (the rows of one device) no expert is named by more than 8 rows; some expert is named by exactly 8 rows of a block.
All inputs are finite; a program needn't handle non-finite values.
Results may differ from the reference program's by a relative error of at most 0.015.
Values may be sent and summed in bfloat16 or wider, within the bound.
A program may use at most 128 MiB of HBM per device.

```python
import math
import jax
import jax.numpy as jnp
import numpy as np
from jax import lax

D = 2048
HEADS = 8
HEAD_QK = 64
HEAD_V = 128
FFE = 1024
GROUPS = 4
TOP = 2
TOKQ = 128
EXPERTS = 64
CAP = 8
TOKA = 12288
TOKB = 32768
N_EP = 64
N_TP = 4


def drawn_pair(key):
    base = jax.random.fold_in(key, 41)
    first, second = jax.random.split(base, 2)
    columns = HEADS * 2 * HEAD_QK
    queries = jnp.clip(jax.random.normal(first, (TOKA, columns), jnp.float32) * 1.3, -6.0, 6.0)
    keys = jnp.clip(jax.random.normal(second, (TOKA, columns), jnp.float32) * 1.3, -6.0, 6.0)
    return (queries, keys)


def draw_query_rows(key, part):
    return drawn_pair(key)[0].astype(jnp.bfloat16)


def draw_key_rows(key, part):
    return drawn_pair(key)[1].astype(jnp.bfloat16)


def steps_of(rng, extent, shards, least, largest):
    factor_of, own = 1.0, jax.random.fold_in(rng, 6)
    for axis_at, shards_of in shards:
        heights = jnp.exp(jax.random.uniform(jax.random.fold_in(own, axis_at), (shards_of,), jnp.float32, least / len(shards), largest / len(shards)))
        factor_of = factor_of * jnp.repeat(heights, extent[axis_at] // shards_of).reshape([-1 if axis == axis_at else 1 for axis in range(len(extent))])
    return factor_of


def routed_block(own_key, own, number, rows, count, top, reach, lean):
    order = jax.random.permutation(own_key, count)
    crowded, usual = shares(count, rows * top, reach, lean, True), shares(count, rows * top, reach, lean, False)
    places = jnp.arange(count)

    def named(sizes, offset_by):
        used = int((sizes > 0).sum())
        fixed = max(1, used // 4)
        moved = fixed + (places - fixed + offset_by * (used - fixed)) % max(1, count - fixed)
        return jnp.zeros((count,), jnp.int32).at[order[jnp.where(places < fixed, places, moved)]].set(jnp.asarray(sizes, jnp.int32))

    sizes = jnp.where(number % 4 == 0, named(crowded, number // 4), named(usual, number - number // 4 - 1))
    mixed = jax.random.permutation(jax.random.fold_in(own, 3), count)
    donor, taker = mixed[0:count // 2 * 2:2], mixed[1:count // 2 * 2:2]
    margin = jnp.minimum(sizes[donor] - 1, reach - sizes[taker]) // 2
    margin = jnp.where((donor == order[0]) | (taker == order[0]) | (sizes[taker] == 0), 0, jnp.maximum(margin, 0))
    moved = jax.random.randint(jax.random.fold_in(own, 4), (count // 2,), 0, 1 << 20) % (margin + 1)
    sizes = sizes.at[donor].add(-moved).at[taker].add(moved)
    members = jnp.searchsorted(jnp.cumsum(sizes), jnp.arange(rows * top), side="right").astype(jnp.int32)
    table = members.reshape(top, rows).T
    table = table[jax.random.permutation(jax.random.fold_in(own, 1), rows)]
    offset_by = jax.random.randint(jax.random.fold_in(own, 2), (rows, 1), 0, top)
    return jnp.take_along_axis(table, (jnp.arange(top)[None, :] + offset_by) % top, axis=1)


def shares(amount, total, bound, skew, full):
    weights = [(1 << 20) // math.isqrt(rank ** skew) + 1 for rank in range(1, amount + 1)]
    largest = bound if full else min(bound, max(-(-total // amount), total * weights[0] // sum(weights)))
    least = 1 if total - largest >= amount - 1 else 0
    given, rest = [largest] + [least] * (amount - 1), total - largest - least * (amount - 1)
    while rest > 0:
        movable = [i for i in range(1, amount) if given[i] < largest] or [i for i in range(1, amount) if given[i] < bound]
        pool, left = sum([weights[i] for i in movable]), rest
        for i in movable:
            addition = min(bound - given[i], max(1, left * weights[i] // pool), rest)
            given[i] = given[i] + addition
            rest = rest - addition
    return np.array(given)


def scatter_about(own_key, extent, width, most, cuts=(), kind=jnp.bfloat16):
    level = steps_of(own_key, extent, cuts, -0.22, 0.18) if cuts else 1.0
    drawn = jax.random.normal(own_key, extent, jnp.float32) * width * level
    return jnp.minimum(jnp.maximum(drawn, -most), most).astype(kind)


def setup_inputs(seed: int = 0) -> dict:
    key_list = jax.random.split(jax.random.key(seed), 15)
    query_rows = draw_query_rows(jax.random.fold_in(key_list[14], 71), 0)
    key_rows = draw_key_rows(jax.random.fold_in(key_list[14], 71), 0)
    value_rows = scatter_about(key_list[2], (TOKA, HEADS * HEAD_V), 1.0, 6.0, ((0, 64), (1, 4)))
    lambdas = jnp.clip(0.3 + 0.5 * jax.random.uniform(key_list[3], (HEADS,), jnp.float32) ** steps_of(key_list[3], (HEADS,), ((0, 4),), -0.2, 0.2), 0.3, 0.8)
    head_gain = jnp.clip(1.0 + 0.18 * jax.random.normal(key_list[4], (HEAD_V,), jnp.float32), 0.1, 1.9)
    w_out = scatter_about(key_list[5], (HEADS * HEAD_V, D), (HEADS * HEAD_V) ** -0.5, 0.1875)
    moe_rows = scatter_about(key_list[6], (TOKB, D), 1.0, 6.0, ((0, 64),))
    ffn_gain = jnp.clip(1.0 + 0.18 * jax.random.normal(key_list[7], (D,), jnp.float32), 0.1, 1.9)
    routes_keys = jax.random.split(jax.random.fold_in(key_list[8], 1), TOKB // TOKQ)
    routes_turns = jax.random.permutation(jax.random.fold_in(key_list[8], 3), TOKB // TOKQ)
    routes = jax.vmap(lambda own, number: routed_block(jax.random.fold_in(key_list[8], 2), own, number, TOKQ, EXPERTS, TOP, CAP, 1))(routes_keys, routes_turns).reshape((TOKB, TOP))
    group_logits = scatter_about(key_list[9], (TOKB, GROUPS), 2.0, 8.0, ((0, 64),), jnp.float32)
    pick_logits = scatter_about(key_list[10], (TOKB, TOP), 1.5, 8.0, ((0, 64),), jnp.float32)
    w_gate = scatter_about(key_list[11], (EXPERTS, D, FFE), D ** -0.5, 0.125, ((0, 64), (2, 4)))
    w_up = scatter_about(key_list[12], (EXPERTS, D, FFE), D ** -0.5, 0.125, ((0, 64), (2, 4)))
    w_down = scatter_about(key_list[13], (EXPERTS, FFE, D), (FFE // 16) ** -0.5, 0.75, ((0, 64), (1, 4)))
    return dict(query_rows=query_rows, key_rows=key_rows, value_rows=value_rows, lambdas=lambdas, head_gain=head_gain, w_out=w_out, moe_rows=moe_rows, ffn_gain=ffn_gain, routes=routes, group_logits=group_logits, pick_logits=pick_logits, w_gate=w_gate, w_up=w_up, w_down=w_down)


EPS = 1e-06
HEAD_SCALE = 0.8

def rms_rows(values, gain):
    squared = lax.optimization_barrier(jnp.mean(values * values, axis=-1, keepdims=True))
    return values * lax.rsqrt(squared + EPS) * gain

def attend(query_rows, key_rows, value_rows, lambdas, head_gain):
    token_count = query_rows.shape[0]
    block_rows = math.gcd(token_count, 128)
    keys = key_rows.astype(jnp.float32).reshape(token_count, HEADS, 2, HEAD_QK)
    values = value_rows.astype(jnp.float32).reshape(token_count, HEADS, HEAD_V)
    queries = query_rows.astype(jnp.float32).reshape(token_count // block_rows, block_rows, HEADS, 2, HEAD_QK)

    def one_block(query_block):
        scores = jnp.einsum('qhmd,khmd->hmqk', query_block, keys, precision=lax.Precision.HIGHEST) * HEAD_QK ** (-0.5)
        weights = jnp.exp(scores - lax.optimization_barrier(jnp.max(scores, axis=-1, keepdims=True)))
        totals = lax.optimization_barrier(jnp.sum(weights, axis=-1))
        rounded = lax.optimization_barrier(weights.astype(jnp.bfloat16)).astype(jnp.float32)
        sums = jnp.einsum('hmqk,khv->hmqv', rounded, values, precision=lax.Precision.HIGHEST)
        per_head = sums[:, 0] / totals[:, 0, :, None] - lambdas[:, None, None] * sums[:, 1] / totals[:, 1, :, None]
        normed = rms_rows(per_head, head_gain) * HEAD_SCALE
        return jnp.transpose(normed, (1, 0, 2)).reshape(block_rows, HEADS * HEAD_V).astype(jnp.bfloat16)
    return lax.map(one_block, queries).reshape(token_count, HEADS * HEAD_V)

def experts_part(moe_rows, ffn_gain, routes, group_logits, pick_logits, w_gate, w_up, w_down):
    model_width = moe_rows.shape[1]
    quarters = N_EP * N_TP
    normed = rms_rows(moe_rows.astype(jnp.float32), ffn_gain).astype(jnp.bfloat16)
    flattened = routes.reshape(quarters, TOKQ * TOP)
    onehot = (flattened[..., None] == jnp.arange(EXPERTS, dtype=jnp.int32)).astype(jnp.int32)
    before = jnp.cumsum(onehot, axis=1) - onehot
    ranking = lax.optimization_barrier(jnp.sum(before * onehot, axis=-1))
    slots = (flattened * quarters + jnp.arange(quarters, dtype=jnp.int32)[:, None]) * CAP + ranking
    source_rows = jnp.repeat(jnp.arange(TOKB, dtype=jnp.int32), TOP)
    buffer_rows = jnp.zeros((EXPERTS * quarters * CAP, model_width), jnp.bfloat16)
    buffer_rows = buffer_rows.at[slots.reshape(-1)].set(normed[source_rows])
    buffer_rows = buffer_rows.reshape(EXPERTS, quarters * CAP, model_width)
    unit_block = FFE // N_TP

    def run_expert(packed):
        expert_rows, gate_weight, up_weight, down_weight = packed
        gate_part = jnp.dot(expert_rows, gate_weight, preferred_element_type=jnp.float32)
        up_part = jnp.dot(expert_rows, up_weight, preferred_element_type=jnp.float32)
        hidden = (jax.nn.silu(gate_part) * up_part).astype(jnp.bfloat16)
        split_hidden = hidden.astype(jnp.float32).reshape(-1, N_TP, unit_block)
        split_down = down_weight.astype(jnp.float32).reshape(N_TP, unit_block, model_width)
        parts = jnp.einsum('rnf,nfd->nrd', split_hidden, split_down, precision=lax.Precision.HIGHEST)
        parts = lax.optimization_barrier(parts.astype(jnp.bfloat16)).astype(jnp.float32)
        return lax.optimization_barrier(jnp.sum(parts, axis=0)).astype(jnp.bfloat16)
    outputs = lax.map(run_expert, (buffer_rows, w_gate, w_up, w_down))
    picked = outputs.reshape(-1, model_width)[slots.reshape(-1)].reshape(TOKB, TOP, model_width)
    group_prob = jax.nn.softmax(group_logits, axis=-1)
    group_index = routes // (EXPERTS // GROUPS)
    matches = (group_index[..., None] == jnp.arange(GROUPS, dtype=jnp.int32)).astype(jnp.float32)
    group_share = lax.optimization_barrier(jnp.sum(group_prob[:, None, :] * matches, axis=-1))
    gate_values = group_share * jax.nn.softmax(pick_logits, axis=-1)
    return lax.optimization_barrier(jnp.sum(gate_values[..., None] * picked.astype(jnp.float32), axis=1)).astype(jnp.bfloat16)

def reference(query_rows, key_rows, value_rows, lambdas, head_gain, w_out, moe_rows, ffn_gain, routes, group_logits, pick_logits, w_gate, w_up, w_down):
    attended = attend(query_rows, key_rows, value_rows, lambdas, head_gain)
    mixer_out = jnp.dot(attended, w_out, preferred_element_type=jnp.float32).astype(jnp.bfloat16)
    moe_out = experts_part(moe_rows, ffn_gain, routes, group_logits, pick_logits, w_gate, w_up, w_down)
    return (mixer_out, moe_out)
```

```python
import jax
import jax.numpy as jnp
from jax import lax
from jax.experimental import pallas as pl
from jax.experimental.pallas import tpu as pltpu
from jax.sharding import PartitionSpec as P

EPS = 1e-06
HEAD_SCALE = 0.8
NZ, NXC, NT = 8, 8, 4
CAP = 8
EXPERTS = 64
ROWS = 192
TOK = 128
D = 2048
HALF = D // 2
UNITS = 256
SLOTS = EXPERTS * CAP
Z_ORDER = (1, 7, 2, 6, 3, 5, 4)
F32 = jnp.float32
BF16 = jnp.bfloat16
MESH = pl.DeviceIdType.MESH


def dot(a, b):
    return lax.dot_general(a, b, (((1,), (0,)), ((), ())), preferred_element_type=F32)


def kernel(
    q_hbm,
    k_hbm,
    v_hbm,
    lam_ref,
    hg_ref,
    wo_hbm,
    moe_hbm,
    fg_ref,
    routes_ref,
    gl_ref,
    pk_ref,
    wg_hbm,
    wu_hbm,
    wd_hbm,
    mix_ref,
    moe_ref,
    qbuf,
    kbuf,
    vbuf,
    psend,
    precv,
    att,
    attall,
    wob,
    xin,
    gmat,
    dsend,
    dmid,
    dout,
    wgb,
    wub,
    wdb,
    hid,
    osend,
    omid,
    oret,
    loc_sem,
    q_ss,
    q_rs,
    k_ss,
    k_rs,
    v_ss,
    v_rs,
    p_ss,
    p_rs,
    a_ss,
    a_rs,
    w_ss,
    w_rs,
    f_ss,
    f_rs,
    d1_ss,
    d1_rs,
    d2_ss,
    d2_rs,
    o1_ss,
    o1_rs,
    o2_ss,
    o2_rs,
):
    ep = lax.axis_index("ep")
    t = lax.axis_index("tp")
    z = ep // NXC
    xc = ep % NXC

    def z_peer(k):
        return ((z + k) % NZ) * NXC + xc

    def xc_peer(j):
        return z * NXC + (xc + j) % NXC

    def remote(src, dst, ssem, rsem, to_ep, to_tp):
        return pltpu.make_async_remote_copy(
            src_ref=src,
            dst_ref=dst,
            send_sem=ssem,
            recv_sem=rsem,
            device_id=(to_ep, to_tp),
            device_id_type=MESH,
        )

    locals_ = [
        (moe_hbm.at[pl.ds(pl.multiple_of(t * TOK, TOK), TOK)], xin),
        (q_hbm, qbuf.at[xc]),
        (k_hbm, kbuf.at[z]),
        (v_hbm, vbuf.at[z]),
        (wg_hbm.at[0], wgb.at[t]),
        (wu_hbm.at[0], wub.at[t]),
        (wd_hbm.at[0, :, pl.ds(0, HALF)], wdb.at[0, t]),
        (wd_hbm.at[0, :, pl.ds(HALF, HALF)], wdb.at[1, t]),
        (wo_hbm, wob),
    ]
    loads = [
        pltpu.make_async_copy(src, dst, loc_sem.at[i]) for i, (src, dst) in enumerate(locals_)
    ]
    for load in loads:
        load.start()

    barrier = pltpu.get_barrier_semaphore()
    for k in range(1, NZ):
        pl.semaphore_signal(barrier, inc=1, device_id=(z_peer(k), t), device_id_type=MESH)
    for j in range(1, NXC):
        pl.semaphore_signal(barrier, inc=1, device_id=(xc_peer(j), t), device_id_type=MESH)
    for y in range(1, NT):
        pl.semaphore_signal(barrier, inc=1, device_id=(ep, (t + y) % NT), device_id_type=MESH)
    pl.semaphore_wait(barrier, NZ - 1 + NXC - 1 + NT - 1)

    right = (t + 1) % NT
    left = (t + 3) % NT

    def w_piece(owner, piece, half=None):
        if piece < 2:
            buf = wgb if piece == 0 else wub
            if half is None:
                return buf.at[owner]
            return buf.at[owner, pl.ds(half * HALF, HALF)]
        if half is None:
            return wdb.at[piece - 2, owner]
        return wdb.at[piece - 2, owner, pl.ds(half * (UNITS // 2), UNITS // 2)]

    def w_source(piece):
        if piece == 0:
            return wg_hbm.at[0]
        if piece == 1:
            return wu_hbm.at[0]
        return wd_hbm.at[0, :, pl.ds((piece - 2) * HALF, HALF)]

    def w_own(way, piece):
        to = right if way == 0 else left
        return remote(
            w_source(piece),
            w_piece(t, piece),
            w_ss.at[way * 4 + piece],
            w_rs.at[way * 4 + piece],
            ep,
            to,
        )

    def w_forward(way, piece):
        owner = left if way == 0 else right
        to = right if way == 0 else left
        return remote(
            w_piece(owner, piece, way),
            w_piece(owner, piece, way),
            f_ss.at[way * 4 + piece],
            f_rs.at[way * 4 + piece],
            ep,
            to,
        )

    def forward_piece(piece):
        for way in range(2):
            w_own(way, piece).wait_recv()
            w_forward(way, piece).start()

    for piece in range(2):
        for way in range(2):
            w_own(way, piece).start()

    def q_copy(j):
        return remote(q_hbm, qbuf.at[xc], q_ss.at[j], q_rs.at[j], xc_peer(j), t)

    def k_copy(k):
        return remote(k_hbm, kbuf.at[z], k_ss.at[k], k_rs.at[k], z_peer(k), t)

    def v_copy(k):
        return remote(v_hbm, vbuf.at[z], v_ss.at[k], v_rs.at[k], z_peer(k), t)

    for j in range(1, NXC):
        q_copy(j).start()
    for k in Z_ORDER:
        k_copy(k).start()
        v_copy(k).start()

    base = pl.multiple_of(t * TOK, TOK)
    picks = routes_ref[pl.ds(base, TOK), :]
    expert_iota = lax.broadcasted_iota(jnp.int32, (TOK, EXPERTS), 1)
    one0 = (picks[:, 0:1] == expert_iota).astype(F32)
    one1 = (picks[:, 1:2] == expert_iota).astype(F32)
    lower = (
        lax.broadcasted_iota(jnp.int32, (TOK, TOK), 1)
        < lax.broadcasted_iota(jnp.int32, (TOK, TOK), 0)
    ).astype(BF16)
    before0 = dot(lower, one0.astype(BF16))
    before1 = dot(lower, one1.astype(BF16)) + jnp.sum(one0, axis=0, keepdims=True)
    rank0 = jnp.sum(before0 * one0, axis=1, keepdims=True)
    rank1 = jnp.sum(before1 * one1, axis=1, keepdims=True)
    slot0 = picks[:, 0:1] * CAP + rank0.astype(jnp.int32)
    slot1 = picks[:, 1:2] * CAP + rank1.astype(jnp.int32)
    slot_iota = lax.broadcasted_iota(jnp.int32, (TOK, SLOTS), 1)
    hit0 = slot_iota == slot0
    hit1 = slot_iota == slot1

    groups = gl_ref[pl.ds(base, TOK), :]
    group_exp = jnp.exp(groups - jnp.max(groups, axis=1, keepdims=True))
    group_prob = group_exp / jnp.sum(group_exp, axis=1, keepdims=True)
    group_iota = lax.broadcasted_iota(jnp.int32, (TOK, 4), 1)
    share0 = jnp.sum(jnp.where((picks[:, 0:1] >> 4) == group_iota, group_prob, 0.0), axis=1, keepdims=True)
    share1 = jnp.sum(jnp.where((picks[:, 1:2] >> 4) == group_iota, group_prob, 0.0), axis=1, keepdims=True)
    pick_logits = pk_ref[pl.ds(base, TOK), :]
    pick_exp = jnp.exp(pick_logits - jnp.max(pick_logits, axis=1, keepdims=True))
    pick_prob = pick_exp / jnp.sum(pick_exp, axis=1, keepdims=True)
    gate0 = share0 * pick_prob[:, 0:1]
    gate1 = share1 * pick_prob[:, 1:2]
    gmat[...] = jnp.where(hit0, gate0, 0.0) + jnp.where(hit1, gate1, 0.0)

    spread = (hit0 | hit1).astype(F32).T.astype(BF16)
    loads[0].wait()
    rows = xin[...].astype(F32)
    squared = jnp.mean(rows * rows, axis=1, keepdims=True)
    xin[...] = (rows * lax.rsqrt(squared + EPS) * fg_ref[...]).astype(BF16)
    for c in range(4):
        cols = pl.ds(c * 512, 512)
        laid = dot(spread, xin[:, cols])
        dsend[:, :, cols] = laid.reshape(EXPERTS, CAP, 512).astype(BF16)

    def d1_copy(k):
        return remote(
            dsend.at[pl.ds(((z + k) % NZ) * NXC, NXC)],
            dmid.at[pl.ds(z * NXC, NXC)],
            d1_ss.at[k],
            d1_rs.at[k],
            z_peer(k),
            t,
        )

    def d2_copy(k, j):
        zs = (z + NZ - k) % NZ
        return remote(
            dmid.at[zs * NXC + (xc + j) % NXC],
            dout.at[zs * NXC + xc],
            d2_ss.at[k * NXC + j],
            d2_rs.at[k * NXC + j],
            xc_peer(j),
            t,
        )

    def o1_copy(h, k):
        return remote(
            osend.at[h, pl.ds(((z + k) % NZ) * NXC, NXC)],
            omid.at[h, pl.ds(z * NXC, NXC)],
            o1_ss.at[h * NZ + k],
            o1_rs.at[h * NZ + k],
            z_peer(k),
            t,
        )

    def o2_copy(h, k, j):
        zs = (z + NZ - k) % NZ
        return remote(
            omid.at[h, zs * NXC + (xc + j) % NXC],
            oret.at[h, zs * NXC + xc],
            o2_ss.at[h * 64 + k * NXC + j],
            o2_rs.at[h * 64 + k * NXC + j],
            xc_peer(j),
            t,
        )

    for k in Z_ORDER:
        d1_copy(k).start()
    dmid[pl.ds(z * NXC, NXC)] = dsend[pl.ds(z * NXC, NXC)]

    def d2_stage(k):
        @pl.loop(1, NXC)
        def _(j):
            d2_copy(k, j).start()

        zs = (z + NZ - k) % NZ
        dout[zs * NXC + xc] = dmid[zs * NXC + xc]

    d2_stage(0)

    forward_piece(0)

    for load in loads[1:4]:
        load.wait()
    for j in range(1, NXC):
        q_copy(j).wait_recv()
    for k in Z_ORDER:
        k_copy(k).wait_recv()
        v_copy(k).wait_recv()

    lane = lax.broadcasted_iota(jnp.int32, (ROWS, 128), 1)

    def p_copy(j):
        return remote(
            psend.at[(xc + j) % NXC], precv.at[xc], p_ss.at[j], p_rs.at[j], xc_peer(j), t
        )

    def attend(j, dst):
        source = (xc + j) % NXC
        stats = jnp.zeros((ROWS, 128), F32)
        for h in range(2):
            cols = pl.ds(h * 128, 128)
            query = qbuf[source, :, cols].astype(F32) * 0.125
            keys = kbuf[:, :, cols].reshape(NZ * ROWS, 128)
            values = vbuf[:, :, cols].reshape(NZ * ROWS, 128)
            for m in range(2):
                own = (lane >= 64) if m else (lane < 64)
                masked = jnp.where(own, query, 0.0).astype(BF16)
                scores = lax.dot_general(
                    masked, keys, (((1,), (1,)), ((), ())), preferred_element_type=F32
                )
                top = jnp.max(scores, axis=1, keepdims=True)
                weights = jnp.exp(scores - top)
                total = jnp.sum(weights, axis=1, keepdims=True)
                summed = dot(weights.astype(BF16), values)
                i = h * 2 + m
                dst[:, pl.ds(i * 128, 128)] = (summed / total).astype(BF16)
                lse = top + jnp.log(total)
                high = lse.astype(BF16).astype(F32)
                mid = (lse - high).astype(BF16).astype(F32)
                low = lse - high - mid
                stats = jnp.where(lane == i, high, stats)
                stats = jnp.where(lane == 4 + i, mid, stats)
                stats = jnp.where(lane == 8 + i, low, stats)
        dst[:, pl.ds(512, 128)] = stats.astype(BF16)

    @pl.loop(1, 5)
    def _(j):
        attend(j, psend.at[(xc + j) % NXC])
        p_copy(j).start()

    forward_piece(1)
    for way in range(2):
        w_own(way, 2).start()

    @pl.loop(5, NXC)
    def _(j):
        attend(j, psend.at[(xc + j) % NXC])
        p_copy(j).start()

    attend(0, precv.at[xc])

    for way in range(2):
        w_own(way, 3).start()

    for k in Z_ORDER:
        d1_copy(k).wait_recv()
        d2_stage(k)

    for j in range(1, NXC):
        p_copy(j).wait_recv()
    lses = []
    for d in range(NXC):
        stats = precv[d, :, pl.ds(512, 128)].astype(F32)
        lses.append(stats + pltpu.roll(stats, 124, 1) + pltpu.roll(stats, 120, 1))
    highest = lses[0]
    for d in range(1, NXC):
        highest = jnp.maximum(highest, lses[d])
    shares = [jnp.exp(lses[d] - highest) for d in range(NXC)]
    whole = shares[0]
    for d in range(1, NXC):
        whole = whole + shares[d]
    for d in range(NXC):
        shares[d] = shares[d] / whole
    for h in range(2):
        mixed = []
        for m in range(2):
            i = h * 2 + m
            acc = jnp.zeros((ROWS, 128), F32)
            for d in range(NXC):
                acc = acc + shares[d][:, i : i + 1] * precv[d, :, pl.ds(i * 128, 128)].astype(F32)
            mixed.append(acc)
        per_head = mixed[0] - lam_ref[h] * mixed[1]
        squared = jnp.mean(per_head * per_head, axis=1, keepdims=True)
        normed = per_head * lax.rsqrt(squared + EPS) * hg_ref[...] * HEAD_SCALE
        for y in range(NT):
            att[y, :, pl.ds(h * 128, 128)] = normed[y * 48 : (y + 1) * 48].astype(BF16)

    def a_copy(y):
        return remote(
            att.at[(t + y) % NT], attall.at[t], a_ss.at[y], a_rs.at[y], ep, (t + y) % NT
        )

    for y in range(1, NT):
        a_copy(y).start()
    attall[t] = att[t]

    forward_piece(2)

    @pl.loop(1, NXC)
    def _(j):
        for k in range(NZ):
            d2_copy(k, j).wait_recv()

    for load in loads[4:6]:
        load.wait()
    for piece in range(2):
        for way in range(2):
            w_forward(way, piece).wait_recv()

    @pl.loop(0, 2)
    def _(r):
        arrived = dout[pl.ds(r * 32, 32)].astype(F32).reshape(256, D).astype(BF16)
        for b in range(NT):
            gate_part = dot(arrived, wgb[b])
            up_part = dot(arrived, wub[b])
            hidden = gate_part / (1.0 + jnp.exp(-gate_part)) * up_part
            hid[pl.ds(pl.multiple_of(r * 256, 256), 256), pl.ds(b * UNITS, UNITS)] = hidden.astype(BF16)

    forward_piece(3)

    def down(h):
        loads[6 + h].wait()
        for way in range(2):
            w_forward(way, 2 + h).wait_recv()

        @pl.loop(0, 2)
        def _(r):
            part = hid[pl.ds(pl.multiple_of(r * 256, 256), 256), :]
            for c in range(2):
                cols = pl.ds(c * 512, 512)
                result = dot(part, wdb[h, :, :, cols].reshape(NT * UNITS, 512))
                osend[h, pl.ds(r * 32, 32), :, cols] = result.reshape(32, CAP, 512).astype(BF16)

        for k in Z_ORDER:
            o1_copy(h, k).start()
        omid[h, pl.ds(z * NXC, NXC)] = osend[h, pl.ds(z * NXC, NXC)]

    def o2_stage(h, k):
        @pl.loop(1, NXC)
        def _(j):
            o2_copy(h, k, j).start()

        zs = (z + NZ - k) % NZ
        oret[h, zs * NXC + xc] = omid[h, zs * NXC + xc]

    down(0)
    o2_stage(0, 0)
    down(1)
    o2_stage(1, 0)

    loads[8].wait()
    for y in range(1, NT):
        a_copy(y).wait_recv()
    for c in range(4):
        cols = pl.ds(c * 512, 512)
        acc = dot(attall[0], wob[pl.ds(0, 256), cols])
        for y in range(1, NT):
            acc = acc + dot(attall[y], wob[pl.ds(y * 256, 256), cols])
        mix_ref[:, cols] = acc.astype(BF16)

    for h in range(2):
        for k in Z_ORDER:
            o1_copy(h, k).wait_recv()
            o2_stage(h, k)

    gates = gmat[...]
    gates_high = gates.astype(BF16)
    gates_low = (gates - gates_high.astype(F32)).astype(BF16)
    for h in range(2):

        @pl.loop(1, NXC)
        def _(j):
            for k in range(NZ):
                o2_copy(h, k, j).wait_recv()

        for c in range(2):
            returned = oret[h, :, :, pl.ds(c * 512, 512)].astype(F32).reshape(SLOTS, 512).astype(BF16)
            result = dot(gates_high, returned) + dot(gates_low, returned)
            moe_ref[:, pl.ds(h * HALF + c * 512, 512)] = result.astype(BF16)

    for j in range(1, NXC):
        q_copy(j).wait_send()
        p_copy(j).wait_send()
    for k in range(1, NZ):
        k_copy(k).wait_send()
        v_copy(k).wait_send()
        d1_copy(k).wait_send()
        for h in range(2):
            o1_copy(h, k).wait_send()
    for y in range(1, NT):
        a_copy(y).wait_send()
    for way in range(2):
        for piece in range(4):
            w_own(way, piece).wait_send()
            w_forward(way, piece).wait_send()

    @pl.loop(1, NXC)
    def _(j):
        for k in range(NZ):
            d2_copy(k, j).wait_send()
            for h in range(2):
                o2_copy(h, k, j).wait_send()


def local(
    query_rows,
    key_rows,
    value_rows,
    lambdas,
    head_gain,
    w_out,
    moe_rows,
    ffn_gain,
    routes,
    group_logits,
    pick_logits,
    w_gate,
    w_up,
    w_down,
):
    any_ = pl.BlockSpec(memory_space=pl.ANY)
    vmem = pl.BlockSpec(memory_space=pltpu.VMEM)
    smem = pl.BlockSpec(memory_space=pltpu.SMEM)
    dma = pltpu.SemaphoreType.DMA
    return pl.pallas_call(
        kernel,
        out_shape=(
            jax.ShapeDtypeStruct((ROWS // NT, D), BF16),
            jax.ShapeDtypeStruct((TOK, D), BF16),
        ),
        in_specs=[any_, any_, any_, smem, vmem, any_, any_, vmem, vmem, vmem, vmem, any_, any_, any_],
        out_specs=(vmem, vmem),
        scratch_shapes=[
            pltpu.VMEM((NXC, ROWS, 256), BF16),
            pltpu.VMEM((NZ, ROWS, 256), BF16),
            pltpu.VMEM((NZ, ROWS, 256), BF16),
            pltpu.VMEM((NXC, ROWS, 640), BF16),
            pltpu.VMEM((NXC, ROWS, 640), BF16),
            pltpu.VMEM((NT, 48, 256), BF16),
            pltpu.VMEM((NT, 48, 256), BF16),
            pltpu.VMEM((1024, D), BF16),
            pltpu.VMEM((TOK, D), BF16),
            pltpu.VMEM((TOK, SLOTS), F32),
            pltpu.VMEM((EXPERTS, CAP, D), BF16),
            pltpu.VMEM((EXPERTS, CAP, D), BF16),
            pltpu.VMEM((EXPERTS, CAP, D), BF16),
            pltpu.VMEM((NT, D, UNITS), BF16),
            pltpu.VMEM((NT, D, UNITS), BF16),
            pltpu.VMEM((2, NT, UNITS, HALF), BF16),
            pltpu.VMEM((SLOTS, 1024), BF16),
            pltpu.VMEM((2, EXPERTS, CAP, HALF), BF16),
            pltpu.VMEM((2, EXPERTS, CAP, HALF), BF16),
            pltpu.VMEM((2, EXPERTS, CAP, HALF), BF16),
            dma((9,)),
            dma((NXC,)),
            dma((NXC,)),
            dma((NZ,)),
            dma((NZ,)),
            dma((NZ,)),
            dma((NZ,)),
            dma((NXC,)),
            dma((NXC,)),
            dma((NT,)),
            dma((NT,)),
            dma((8,)),
            dma((8,)),
            dma((8,)),
            dma((8,)),
            dma((NZ,)),
            dma((NZ,)),
            dma((64,)),
            dma((64,)),
            dma((2 * NZ,)),
            dma((2 * NZ,)),
            dma((128,)),
            dma((128,)),
        ],
        compiler_params=pltpu.CompilerParams(
            collective_id=0, has_side_effects=True, vmem_limit_bytes=66_000_000
        ),
    )(
        query_rows,
        key_rows,
        value_rows,
        lambdas,
        head_gain[None],
        w_out,
        moe_rows,
        ffn_gain[None],
        routes,
        group_logits,
        pick_logits,
        w_gate,
        w_up,
        w_down,
    )


def solution(mesh):
    return jax.shard_map(
        local,
        mesh=mesh,
        in_specs=(
            P("ep", "tp"),
            P("ep", "tp"),
            P("ep", "tp"),
            P("tp"),
            P(),
            P(),
            P("ep", None),
            P(),
            P("ep", None),
            P("ep", None),
            P("ep", None),
            P("ep", None, "tp"),
            P("ep", None, "tp"),
            P("ep", "tp", None),
        ),
        out_specs=(P(("ep", "tp"), None), P(("ep", "tp"), None)),
        check_vma=False,
    )
```

```python
import jax
import jax.numpy as jnp
from jax import lax
from jax.experimental import pallas as pl
from jax.experimental.pallas import tpu as pltpu
from jax.sharding import PartitionSpec as P

EPS = 1e-06
HEAD_SCALE = 0.8
NZ, NXC, NT = 8, 8, 4
CAP = 8
EXPERTS = 64
ROWS = 192
TOK = 128
D = 2048
HALF = D // 2
NCH = 8
CW = D // NCH
UNITS = 256
SLOTS = EXPERTS * CAP
Z_ORDER = (1, 7, 2, 6, 3, 5, 4)
F32 = jnp.float32
BF16 = jnp.bfloat16
MESH = pl.DeviceIdType.MESH


def dot(a, b):
    return lax.dot_general(a, b, (((1,), (0,)), ((), ())), preferred_element_type=F32)


def kernel(
    q_hbm,
    k_hbm,
    v_hbm,
    lam_ref,
    hg_ref,
    wo_hbm,
    moe_hbm,
    fg_ref,
    routes_ref,
    gl_ref,
    pk_ref,
    wg_hbm,
    wu_hbm,
    wd_hbm,
    mix_ref,
    moe_ref,
    qbuf,
    kbuf,
    vbuf,
    psend,
    precv,
    att,
    attall,
    wob,
    xin,
    gmat,
    dsend,
    dmid,
    dout,
    xall,
    wgb,
    wub,
    wdb,
    hid,
    osend,
    omid,
    oret,
    loc_sem,
    q_ss,
    q_rs,
    kv_ss,
    kv_rs,
    p_ss,
    p_rs,
    a_ss,
    a_rs,
    w_ss,
    w_rs,
    f_ss,
    f_rs,
    d1_ss,
    d1_rs,
    d2_ss,
    d2_rs,
    o1_ss,
    o1_rs,
    o2_ss,
    o2_rs,
):
    ep = lax.axis_index("ep")
    t = lax.axis_index("tp")
    z = ep // NXC
    xc = ep % NXC

    def z_peer(k):
        return ((z + k) % NZ) * NXC + xc

    def xc_peer(j):
        return z * NXC + (xc + j) % NXC

    def remote(src, dst, ssem, rsem, to_ep, to_tp):
        return pltpu.make_async_remote_copy(
            src_ref=src,
            dst_ref=dst,
            send_sem=ssem,
            recv_sem=rsem,
            device_id=(to_ep, to_tp),
            device_id_type=MESH,
        )
    base = pl.multiple_of(t * TOK, TOK)
    locals_ = [
        (moe_hbm.at[pl.ds(base, TOK)], xin),
        (q_hbm, qbuf.at[xc]),
        (k_hbm, kbuf.at[z]),
        (v_hbm, vbuf.at[z]),
        (wg_hbm.at[0], wgb.at[t]),
        (wu_hbm.at[0], wub.at[t]),
        (wo_hbm, wob),
    ] + [(wd_hbm.at[0, :, pl.ds(h * CW, CW)], wdb.at[h, t]) for h in range(NCH)]
    loads = [
        pltpu.make_async_copy(src, dst, loc_sem.at[i]) for i, (src, dst) in enumerate(locals_)
    ]
    for load in loads:
        load.start()

    barrier = pltpu.get_barrier_semaphore()
    for k in range(1, NZ):
        pl.semaphore_signal(barrier, inc=1, device_id=(z_peer(k), t), device_id_type=MESH)
    for j in range(1, NXC):
        pl.semaphore_signal(barrier, inc=1, device_id=(xc_peer(j), t), device_id_type=MESH)
    for y in range(1, NT):
        pl.semaphore_signal(barrier, inc=1, device_id=(ep, (t + y) % NT), device_id_type=MESH)
    mine = pl.ds(base, TOK)
    pick0 = routes_ref[0:1, mine]
    pick1 = routes_ref[1:2, mine]
    expert_iota = lax.broadcasted_iota(jnp.int32, (EXPERTS, TOK), 0)
    one0 = (pick0 == expert_iota).astype(F32)
    one1 = (pick1 == expert_iota).astype(F32)
    earlier = (
        lax.broadcasted_iota(jnp.int32, (TOK, TOK), 0)
        < lax.broadcasted_iota(jnp.int32, (TOK, TOK), 1)
    ).astype(BF16)
    before0 = dot(one0.astype(BF16), earlier)
    before1 = dot(one1.astype(BF16), earlier) + jnp.sum(one0, axis=1, keepdims=True)
    rank0 = jnp.sum(before0 * one0, axis=0, keepdims=True)
    rank1 = jnp.sum(before1 * one1, axis=0, keepdims=True)
    slot_iota = lax.broadcasted_iota(jnp.int32, (SLOTS, TOK), 0)
    hit0 = slot_iota == pick0 * CAP + rank0.astype(jnp.int32)
    hit1 = slot_iota == pick1 * CAP + rank1.astype(jnp.int32)

    spread = (hit0 | hit1).astype(F32).astype(BF16)
    loads[0].wait()
    rows = xin[...].astype(F32)
    squared = jnp.mean(rows * rows, axis=1, keepdims=True)
    xin[...] = (rows * lax.rsqrt(squared + EPS) * fg_ref[...]).astype(BF16)
    for c in range(4):
        cols = pl.ds(c * 512, 512)
        laid = dot(spread, xin[:, cols])
        dsend[:, :, cols] = laid.reshape(EXPERTS, CAP, 512).astype(BF16)

    groups = gl_ref[:, mine]
    group_exp = jnp.exp(groups - jnp.max(groups, axis=0, keepdims=True))
    group_prob = group_exp / jnp.sum(group_exp, axis=0, keepdims=True)
    group_iota = lax.broadcasted_iota(jnp.int32, (4, TOK), 0)
    share0 = jnp.sum(jnp.where((pick0 >> 4) == group_iota, group_prob, 0.0), axis=0, keepdims=True)
    share1 = jnp.sum(jnp.where((pick1 >> 4) == group_iota, group_prob, 0.0), axis=0, keepdims=True)
    pick_logits = pk_ref[:, mine]
    pick_exp = jnp.exp(pick_logits - jnp.max(pick_logits, axis=0, keepdims=True))
    pick_prob = pick_exp / jnp.sum(pick_exp, axis=0, keepdims=True)
    gate0 = share0 * pick_prob[0:1]
    gate1 = share1 * pick_prob[1:2]
    gates = (jnp.where(hit0, gate0, 0.0) + jnp.where(hit1, gate1, 0.0)).T
    gates_high = gates.astype(BF16)
    gmat[pl.ds(0, TOK), :] = gates_high
    gmat[pl.ds(TOK, TOK), :] = (gates - gates_high.astype(F32)).astype(BF16)
    pl.semaphore_wait(barrier, NZ - 1 + NXC - 1 + NT - 1)

    right = (t + 1) % NT
    left = (t + 3) % NT

    def w_piece(owner, piece, half=None):
        if piece < 2:
            buf = wgb if piece == 0 else wub
            if half is None:
                return buf.at[owner]
            return buf.at[owner, pl.ds(half * HALF, HALF)]
        if half is None:
            return wdb.at[piece - 2, owner]
        return wdb.at[piece - 2, owner, pl.ds(half * (UNITS // 2), UNITS // 2)]

    def w_source(piece):
        if piece == 0:
            return wg_hbm.at[0]
        if piece == 1:
            return wu_hbm.at[0]
        return wd_hbm.at[0, :, pl.ds((piece - 2) * CW, CW)]

    def w_own(way, piece):
        to = right if way == 0 else left
        return remote(
            w_source(piece),
            w_piece(t, piece),
            w_ss.at[way * (2 + NCH) + piece],
            w_rs.at[way * (2 + NCH) + piece],
            ep,
            to,
        )

    def w_forward(way, piece):
        owner = left if way == 0 else right
        to = right if way == 0 else left
        return remote(
            w_piece(owner, piece, way),
            w_piece(owner, piece, way),
            f_ss.at[way * (2 + NCH) + piece],
            f_rs.at[way * (2 + NCH) + piece],
            ep,
            to,
        )

    def send_piece(piece):
        for way in range(2):
            w_own(way, piece).start()

    def forward_piece(piece):
        for way in range(2):
            w_own(way, piece).wait_recv()
            w_forward(way, piece).start()

    def q_copy(j):
        return remote(q_hbm, qbuf.at[xc], q_ss.at[j], q_rs.at[j], xc_peer(j), t)

    def kv_copy(way, step, which):
        shift = 1 - step if way == 0 else step - 1
        slot = (z + NZ + shift) % NZ
        buf = vbuf if which else kbuf
        src = (v_hbm if which else k_hbm) if step == 1 else buf.at[slot]
        i = (way * 5 + step) * 2 + which
        return remote(
            src, buf.at[slot], kv_ss.at[i], kv_rs.at[i], z_peer(1 if way == 0 else NZ - 1), t
        )

    def kv_parts(step):
        if step < 4:
            return [(0, 0), (0, 1), (1, 0), (1, 1)]
        return [(0, 0), (1, 1)]
    send_piece(0)
    send_piece(1)
    for way, which in kv_parts(1):
        kv_copy(way, 1, which).start()
    for j in range(1, NXC):
        q_copy(j).start()

    def d1_copy(k):
        return remote(
            dsend.at[pl.ds(((z + k) % NZ) * NXC, NXC)],
            dmid.at[pl.ds(z * NXC, NXC)],
            d1_ss.at[k],
            d1_rs.at[k],
            z_peer(k),
            t,
        )

    def d2_copy(k, j):
        zs = (z + NZ - k) % NZ
        return remote(
            dmid.at[zs * NXC + (xc + j) % NXC],
            dout.at[zs * NXC + xc],
            d2_ss.at[0],
            d2_rs.at[j],
            xc_peer(j),
            t,
        )

    def o1_copy(h, k):
        return remote(
            osend.at[h, pl.ds(((z + k) % NZ) * NXC, NXC)],
            omid.at[h, pl.ds(z * NXC, NXC)],
            o1_ss.at[h * NZ + k],
            o1_rs.at[h * NZ + k],
            z_peer(k),
            t,
        )

    def o2_copy(h, k, j):
        zs = (z + NZ - k) % NZ
        return remote(
            omid.at[h, zs * NXC + (xc + j) % NXC],
            oret.at[h, zs * NXC + xc],
            o2_ss.at[h],
            o2_rs.at[h * NXC + j],
            xc_peer(j),
            t,
        )

    def d2_whole(j, count):
        return remote(
            dmid.at[pl.ds(0, count)],
            dout.at[pl.ds(0, count)],
            d2_ss.at[0],
            d2_rs.at[j],
            xc_peer(j),
            t,
        )

    def o2_whole(h, j, count):
        return remote(
            omid.at[h, pl.ds(0, count)],
            oret.at[h, pl.ds(0, count)],
            o2_ss.at[h],
            o2_rs.at[h * NXC + j],
            xc_peer(j),
            t,
        )

    def d2_stage(k):
        if k:
            d1_copy(k).wait_recv()

        @pl.loop(1, NXC)
        def _(j):
            d2_copy(k, j).start()

        zs = (z + NZ - k) % NZ
        dout[zs * NXC + xc] = dmid[zs * NXC + xc]

    dmid[pl.ds(z * NXC, NXC)] = dsend[pl.ds(z * NXC, NXC)]

    for step in range(1, 5):
        for way, which in kv_parts(step):
            kv_copy(way, step, which).wait_recv()
        if step < 4:
            for way, which in kv_parts(step + 1):
                kv_copy(way, step + 1, which).start()
        if step == 3:
            for k in Z_ORDER:
                d1_copy(k).start()

    for load in loads[1:4]:
        load.wait()
    for j in range(1, NXC):
        q_copy(j).wait_recv()

    lane = lax.broadcasted_iota(jnp.int32, (ROWS, 128), 1)

    def p_copy(j):
        return remote(
            psend.at[(xc + j) % NXC], precv.at[xc], p_ss.at[j], p_rs.at[j], xc_peer(j), t
        )

    def attend(j, dst):
        source = (xc + j) % NXC
        stats = jnp.zeros((ROWS, 128), F32)
        for h in range(2):
            cols = pl.ds(h * 128, 128)
            query = qbuf[source, :, cols].astype(F32) * 0.125
            keys = kbuf[:, :, cols].reshape(NZ * ROWS, 128)
            values = vbuf[:, :, cols].reshape(NZ * ROWS, 128)
            for m in range(2):
                own = (lane >= 64) if m else (lane < 64)
                masked = jnp.where(own, query, 0.0).astype(BF16)
                scores = lax.dot_general(
                    masked, keys, (((1,), (1,)), ((), ())), preferred_element_type=F32
                )
                top = jnp.max(scores, axis=1, keepdims=True)
                weights = jnp.exp(scores - top)
                total = jnp.sum(weights, axis=1, keepdims=True)
                summed = dot(weights.astype(BF16), values)
                i = h * 2 + m
                dst[:, pl.ds(i * 128, 128)] = (summed / total).astype(BF16)
                lse = top + jnp.log(total)
                high = lse.astype(BF16).astype(F32)
                mid = (lse - high).astype(BF16).astype(F32)
                low = lse - high - mid
                stats = jnp.where(lane == i, high, stats)
                stats = jnp.where(lane == 4 + i, mid, stats)
                stats = jnp.where(lane == 8 + i, low, stats)
        dst[:, pl.ds(512, 128)] = stats.astype(BF16)

    def attend_range(first, last):
        @pl.loop(first, last)
        def _(j):
            attend(j, psend.at[(xc + j) % NXC])
            p_copy(j).start()
    attend_range(1, 3)
    d2_stage(0)
    forward_piece(0)
    attend_range(3, 6)
    d2_stage(1)
    d2_stage(7)
    send_piece(2)
    send_piece(3)
    attend_range(6, NXC)
    attend(0, precv.at[xc])
    forward_piece(1)
    d2_stage(2)
    d2_stage(6)
    for j in range(1, NXC):
        p_copy(j).wait_recv()
    d2_stage(3)
    d2_stage(5)
    lses = []
    for d in range(NXC):
        stats = precv[d, :, pl.ds(512, 128)].astype(F32)
        lses.append(stats + pltpu.roll(stats, 124, 1) + pltpu.roll(stats, 120, 1))
    highest = lses[0]
    for d in range(1, NXC):
        highest = jnp.maximum(highest, lses[d])
    shares = [jnp.exp(lses[d] - highest) for d in range(NXC)]
    whole = shares[0]
    for d in range(1, NXC):
        whole = whole + shares[d]
    for d in range(NXC):
        shares[d] = shares[d] / whole
    for h in range(2):
        mixed = []
        for m in range(2):
            i = h * 2 + m
            acc = jnp.zeros((ROWS, 128), F32)
            for d in range(NXC):
                acc = acc + shares[d][:, i : i + 1] * precv[d, :, pl.ds(i * 128, 128)].astype(F32)
            mixed.append(acc)
        per_head = mixed[0] - lam_ref[h] * mixed[1]
        squared = jnp.mean(per_head * per_head, axis=1, keepdims=True)
        normed = per_head * lax.rsqrt(squared + EPS) * hg_ref[...] * HEAD_SCALE
        for y in range(NT):
            att[y, :, pl.ds(h * 128, 128)] = normed[y * 48 : (y + 1) * 48].astype(BF16)

    def a_copy(y):
        return remote(
            att.at[(t + y) % NT], attall.at[t], a_ss.at[y], a_rs.at[y], ep, (t + y) % NT
        )

    for y in range(1, NT):
        a_copy(y).start()
    attall[t] = att[t]
    d2_stage(4)
    forward_piece(2)
    forward_piece(3)
    send_piece(4)
    send_piece(5)
    for j in range(1, NXC):
        d2_whole(j, NZ).wait_recv()

    for load in loads[4:6]:
        load.wait()

    def hidden_block(r, off):
        b = (t + off) % NT
        arrived = xall[pl.ds(pl.multiple_of(r * 256, 256), 256), :]
        gate_part = dot(arrived, wgb[b])
        up_part = dot(arrived, wub[b])
        hidden = gate_part / (1.0 + jnp.exp(-gate_part)) * up_part
        hid[
            pl.ds(pl.multiple_of(r * 256, 256), 256), pl.ds(pl.multiple_of(b * UNITS, UNITS), UNITS)
        ] = hidden.astype(BF16)
    @pl.loop(0, 2)
    def _(r):
        xall[pl.ds(pl.multiple_of(r * 256, 256), 256), :] = dout[pl.ds(r * 32, 32)].reshape(256, D)
        for off in (0, 1, 3):
            hidden_block(r, off)
    for piece in range(2):
        for way in range(2):
            w_forward(way, piece).wait_recv()
    @pl.loop(0, 2)
    def _(r):
        hidden_block(r, 2)

    def down(h):
        loads[7 + h].wait()
        for way in range(2):
            w_forward(way, 2 + h).wait_recv()

        @pl.loop(0, 2)
        def _(r):
            part = hid[pl.ds(pl.multiple_of(r * 256, 256), 256), :]
            result = dot(part, wdb[h].reshape(NT * UNITS, CW))
            osend[h, pl.ds(r * 32, 32)] = result.reshape(32, CAP, CW).astype(BF16)

        for k in Z_ORDER:
            o1_copy(h, k).start()
        omid[h, pl.ds(z * NXC, NXC)] = osend[h, pl.ds(z * NXC, NXC)]

    def o2_stage(h, k):
        if k:
            o1_copy(h, k).wait_recv()

        @pl.loop(1, NXC)
        def _(j):
            o2_copy(h, k, j).start()

        zs = (z + NZ - k) % NZ
        oret[h, zs * NXC + xc] = omid[h, zs * NXC + xc]

    def o2_stages(h):
        for k in (0,) + Z_ORDER:
            o2_stage(h, k)

    def combine(h):
        for j in range(1, NXC):
            o2_whole(h, j, NZ).wait_recv()

        result = dot(gmat[...], oret[h].reshape(SLOTS, CW))
        moe_ref[:, pl.ds(h * CW, CW)] = (result[:TOK] + result[TOK:]).astype(BF16)

    def project():
        loads[6].wait()
        for y in range(1, NT):
            a_copy(y).wait_recv()
        for c in range(4):
            cols = pl.ds(c * 512, 512)
            acc = dot(attall[0], wob[pl.ds(0, 256), cols])
            for y in range(1, NT):
                acc = acc + dot(attall[y], wob[pl.ds(y * 256, 256), cols])
            mix_ref[:, cols] = acc.astype(BF16)

    for h in range(NCH):
        down(h)
        if h + 2 < NCH:
            forward_piece(2 + h + 2)
        if h + 4 < NCH:
            send_piece(2 + h + 4)
        if h >= 2:
            o2_stages(h - 2)
        if h >= 4:
            combine(h - 4)
    project()
    o2_stages(NCH - 2)
    combine(NCH - 4)
    combine(NCH - 3)
    o2_stages(NCH - 1)
    combine(NCH - 2)
    combine(NCH - 1)
    for j in range(1, NXC):
        q_copy(j).wait_send()
        p_copy(j).wait_send()
    for step in range(1, 5):
        for way, which in kv_parts(step):
            kv_copy(way, step, which).wait_send()
    for k in range(1, NZ):
        d1_copy(k).wait_send()
        for h in range(NCH):
            o1_copy(h, k).wait_send()
    for y in range(1, NT):
        a_copy(y).wait_send()
    for way in range(2):
        for piece in range(2 + NCH):
            w_own(way, piece).wait_send()
            w_forward(way, piece).wait_send()

    d2_whole(1, 56).wait_send()
    for h in range(NCH):
        o2_whole(h, 1, 56).wait_send()


def local(
    query_rows,
    key_rows,
    value_rows,
    lambdas,
    head_gain,
    w_out,
    moe_rows,
    ffn_gain,
    routes,
    group_logits,
    pick_logits,
    w_gate,
    w_up,
    w_down,
):
    any_ = pl.BlockSpec(memory_space=pl.ANY)
    vmem = pl.BlockSpec(memory_space=pltpu.VMEM)
    smem = pl.BlockSpec(memory_space=pltpu.SMEM)
    dma = pltpu.SemaphoreType.DMA
    return pl.pallas_call(
        kernel,
        out_shape=(
            jax.ShapeDtypeStruct((ROWS // NT, D), BF16),
            jax.ShapeDtypeStruct((TOK, D), BF16),
        ),
        in_specs=[any_, any_, any_, smem, vmem, any_, any_, vmem, vmem, vmem, vmem, any_, any_, any_],
        out_specs=(vmem, vmem),
        scratch_shapes=[
            pltpu.VMEM((NXC, ROWS, 256), BF16),
            pltpu.VMEM((NZ, ROWS, 256), BF16),
            pltpu.VMEM((NZ, ROWS, 256), BF16),
            pltpu.VMEM((NXC, ROWS, 640), BF16),
            pltpu.VMEM((NXC, ROWS, 640), BF16),
            pltpu.VMEM((NT, 48, 256), BF16),
            pltpu.VMEM((NT, 48, 256), BF16),
            pltpu.VMEM((1024, D), BF16),
            pltpu.VMEM((TOK, D), BF16),
            pltpu.VMEM((2 * TOK, SLOTS), BF16),
            pltpu.VMEM((EXPERTS, CAP, D), BF16),
            pltpu.VMEM((EXPERTS, CAP, D), BF16),
            pltpu.VMEM((EXPERTS, CAP, D), BF16),
            pltpu.VMEM((SLOTS, D), BF16),
            pltpu.VMEM((NT, D, UNITS), BF16),
            pltpu.VMEM((NT, D, UNITS), BF16),
            pltpu.VMEM((NCH, NT, UNITS, CW), BF16),
            pltpu.VMEM((SLOTS, 1024), BF16),
            pltpu.VMEM((NCH, EXPERTS, CAP, CW), BF16),
            pltpu.VMEM((NCH, EXPERTS, CAP, CW), BF16),
            pltpu.VMEM((NCH, EXPERTS, CAP, CW), BF16),
            dma((15,)),
            dma((NXC,)),
            dma((NXC,)),
            dma((20,)),
            dma((20,)),
            dma((NXC,)),
            dma((NXC,)),
            dma((NT,)),
            dma((NT,)),
            dma((2 * (2 + NCH),)),
            dma((2 * (2 + NCH),)),
            dma((2 * (2 + NCH),)),
            dma((2 * (2 + NCH),)),
            dma((NZ,)),
            dma((NZ,)),
            dma((1,)),
            dma((NXC,)),
            dma((NCH * NZ,)),
            dma((NCH * NZ,)),
            dma((NCH,)),
            dma((NCH * NXC,)),
        ],
        compiler_params=pltpu.CompilerParams(
            collective_id=0, has_side_effects=True, vmem_limit_bytes=66_000_000
        ),
    )(
        query_rows,
        key_rows,
        value_rows,
        lambdas,
        head_gain[None],
        w_out,
        moe_rows,
        ffn_gain[None],
        routes.T,
        group_logits.T,
        pick_logits.T,
        w_gate,
        w_up,
        w_down,
    )


def solution(mesh):
    return jax.shard_map(
        local,
        mesh=mesh,
        in_specs=(
            P("ep", "tp"),
            P("ep", "tp"),
            P("ep", "tp"),
            P("tp"),
            P(),
            P(),
            P("ep", None),
            P(),
            P("ep", None),
            P("ep", None),
            P("ep", None),
            P("ep", None, "tp"),
            P("ep", None, "tp"),
            P("ep", "tp", None),
        ),
        out_specs=(P(("ep", "tp"), None), P(("ep", "tp"), None)),
        check_vma=False,
    )
```

```python
import jax
import jax.numpy as jnp
from jax import lax
from jax.experimental import pallas as pl
from jax.experimental.pallas import tpu as pltpu
from jax.sharding import PartitionSpec as P

EPS = 1e-06
HEAD_SCALE = 0.8
NZ, NXC, NT = 8, 8, 4
CAP = 8
EXPERTS = 64
ROWS = 192
TOK = 128
D = 2048
HALF = D // 2
NCH = 8
CW = D // NCH
UNITS = 256
SLOTS = EXPERTS * CAP
Z_ORDER = (1, 7, 2, 6, 3, 5, 4)
ROW_ORDER = (0,) + Z_ORDER
NEAR = ROW_ORDER[:5]
ZROWS = NXC * CAP
F32 = jnp.float32
BF16 = jnp.bfloat16
MESH = pl.DeviceIdType.MESH


def dot(a, b):
    return lax.dot_general(a, b, (((1,), (0,)), ((), ())), preferred_element_type=F32)


def kernel(
    q_hbm,
    k_hbm,
    v_hbm,
    lam_ref,
    hg_ref,
    wo_hbm,
    moe_hbm,
    fg_ref,
    routes_ref,
    gl_ref,
    pk_ref,
    wg_hbm,
    wu_hbm,
    wd_hbm,
    mix_ref,
    moe_ref,
    qbuf,
    kbuf,
    vbuf,
    psend,
    precv,
    att,
    attall,
    wob,
    xin,
    gmat,
    dsend,
    dmid,
    dout,
    xall,
    wgb,
    wub,
    wdb,
    hid,
    osend,
    omid,
    oret,
    loc_sem,
    q_ss,
    q_rs,
    kv_ss,
    kv_rs,
    p_ss,
    p_rs,
    a_ss,
    a_rs,
    w_ss,
    w_rs,
    f_ss,
    f_rs,
    d1_ss,
    d1_rs,
    d2_ss,
    d2_rs,
    o1_ss,
    o1_rs,
    o2_ss,
    o2_rs,
):
    ep = lax.axis_index("ep")
    t = lax.axis_index("tp")
    z = ep // NXC
    xc = ep % NXC
    core = ep % 2

    def z_peer(k):
        return ((z + k) % NZ) * NXC + xc

    def xc_peer(j):
        return z * NXC + (xc + j) % NXC

    def remote(src, dst, ssem, rsem, to_ep, to_tp):
        return pltpu.make_async_remote_copy(
            src_ref=src,
            dst_ref=dst,
            send_sem=ssem,
            recv_sem=rsem,
            device_id=(to_ep, to_tp),
            device_id_type=MESH,
        )
    base = pl.multiple_of(t * TOK, TOK)
    locals_ = [
        (moe_hbm.at[pl.ds(base, TOK)], xin),
        (q_hbm, qbuf.at[xc]),
        (k_hbm, kbuf.at[z]),
        (v_hbm, vbuf.at[z]),
        (wg_hbm.at[0], wgb.at[t]),
        (wu_hbm.at[0], wub.at[t]),
        (wo_hbm, wob),
    ] + [(wd_hbm.at[0, :, pl.ds(h * CW, CW)], wdb.at[h, t]) for h in range(NCH)]
    loads = [
        pltpu.make_async_copy(src, dst, loc_sem.at[i]) for i, (src, dst) in enumerate(locals_)
    ]
    for load in loads:
        load.start()

    barrier = pltpu.get_barrier_semaphore()
    for k in range(1, NZ):
        pl.semaphore_signal(barrier, inc=1, device_id=(z_peer(k), t), device_id_type=MESH)
    for j in range(1, NXC):
        pl.semaphore_signal(barrier, inc=1, device_id=(xc_peer(j), t), device_id_type=MESH)
    for y in range(1, NT):
        pl.semaphore_signal(barrier, inc=1, device_id=(ep, (t + y) % NT), device_id_type=MESH)
    mine = pl.ds(base, TOK)
    pick0 = routes_ref[0:1, mine]
    pick1 = routes_ref[1:2, mine]
    expert_iota = lax.broadcasted_iota(jnp.int32, (EXPERTS, TOK), 0)
    one0 = (pick0 == expert_iota).astype(F32)
    one1 = (pick1 == expert_iota).astype(F32)
    earlier = (
        lax.broadcasted_iota(jnp.int32, (TOK, TOK), 0)
        < lax.broadcasted_iota(jnp.int32, (TOK, TOK), 1)
    ).astype(BF16)
    before0 = dot(one0.astype(BF16), earlier)
    before1 = dot(one1.astype(BF16), earlier) + jnp.sum(one0, axis=1, keepdims=True)
    rank0 = jnp.sum(before0 * one0, axis=0, keepdims=True)
    rank1 = jnp.sum(before1 * one1, axis=0, keepdims=True)
    slot_iota = lax.broadcasted_iota(jnp.int32, (SLOTS, TOK), 0)
    hit0 = slot_iota == pick0 * CAP + rank0.astype(jnp.int32)
    hit1 = slot_iota == pick1 * CAP + rank1.astype(jnp.int32)

    spread = (hit0 | hit1).astype(F32).astype(BF16)
    loads[0].wait()
    rows = xin[...].astype(F32)
    squared = jnp.mean(rows * rows, axis=1, keepdims=True)
    xin[...] = (rows * lax.rsqrt(squared + EPS) * fg_ref[...]).astype(BF16)
    for c in range(4):
        cols = pl.ds(c * 512, 512)
        laid = dot(spread, xin[:, cols])
        dsend[:, :, cols] = laid.reshape(EXPERTS, CAP, 512).astype(BF16)

    groups = gl_ref[:, mine]
    group_exp = jnp.exp(groups - jnp.max(groups, axis=0, keepdims=True))
    group_prob = group_exp / jnp.sum(group_exp, axis=0, keepdims=True)
    group_iota = lax.broadcasted_iota(jnp.int32, (4, TOK), 0)
    share0 = jnp.sum(jnp.where((pick0 >> 4) == group_iota, group_prob, 0.0), axis=0, keepdims=True)
    share1 = jnp.sum(jnp.where((pick1 >> 4) == group_iota, group_prob, 0.0), axis=0, keepdims=True)
    pick_logits = pk_ref[:, mine]
    pick_exp = jnp.exp(pick_logits - jnp.max(pick_logits, axis=0, keepdims=True))
    pick_prob = pick_exp / jnp.sum(pick_exp, axis=0, keepdims=True)
    gate0 = share0 * pick_prob[0:1]
    gate1 = share1 * pick_prob[1:2]
    gates = (jnp.where(hit0, gate0, 0.0) + jnp.where(hit1, gate1, 0.0)).T
    gates_high = gates.astype(BF16)
    gmat[pl.ds(0, TOK), :] = gates_high
    gmat[pl.ds(TOK, TOK), :] = (gates - gates_high.astype(F32)).astype(BF16)
    pl.semaphore_wait(barrier, NZ - 1 + NXC - 1 + NT - 1)

    right = (t + 1) % NT
    left = (t + 3) % NT

    def w_piece(owner, piece, half=None):
        if piece < 2:
            buf = wgb if piece == 0 else wub
            if half is None:
                return buf.at[owner]
            return buf.at[owner, pl.ds(half * HALF, HALF)]
        if half is None:
            return wdb.at[piece - 2, owner]
        return wdb.at[piece - 2, owner, pl.ds(half * (UNITS // 2), UNITS // 2)]

    def w_source(piece):
        if piece == 0:
            return wg_hbm.at[0]
        if piece == 1:
            return wu_hbm.at[0]
        return wd_hbm.at[0, :, pl.ds((piece - 2) * CW, CW)]

    def w_own(way, piece):
        to = right if way == 0 else left
        return remote(
            w_source(piece),
            w_piece(t, piece),
            w_ss.at[way * (2 + NCH) + piece],
            w_rs.at[way * (2 + NCH) + piece],
            ep,
            to,
        )

    def w_forward(way, piece):
        owner = left if way == 0 else right
        to = right if way == 0 else left
        return remote(
            w_piece(owner, piece, way),
            w_piece(owner, piece, way),
            f_ss.at[way * (2 + NCH) + piece],
            f_rs.at[way * (2 + NCH) + piece],
            ep,
            to,
        )

    def send_piece(piece):
        for way in range(2):
            w_own(way, piece).start()

    def forward_piece(piece):
        for way in range(2):
            w_own(way, piece).wait_recv()
            w_forward(way, piece).start()

    def q_copy(j):
        return remote(q_hbm, qbuf.at[xc], q_ss.at[j], q_rs.at[j], xc_peer(j), t)

    def kv_copy(way, step, which):
        shift = 1 - step if way == 0 else step - 1
        slot = (z + NZ + shift) % NZ
        buf = vbuf if which else kbuf
        src = (v_hbm if which else k_hbm) if step == 1 else buf.at[slot]
        i = (way * 5 + step) * 2 + which
        return remote(
            src, buf.at[slot], kv_ss.at[i], kv_rs.at[i], z_peer(1 if way == 0 else NZ - 1), t
        )

    def d1_part(k, part):
        return remote(
            dsend.at[pl.ds(((z + k) % NZ) * NXC + part * 2, 2)],
            dmid.at[pl.ds(z * NXC + part * 2, 2)],
            d1_ss.at[k],
            d1_rs.at[k],
            z_peer(k),
            t,
        )

    def d1_parts(part):
        d1_part(1, part).start()
        d1_part(7, part).start()

    def kv_parts(step):
        if step < 4:
            return [(0, 0), (0, 1), (1, 0), (1, 1)]
        return [(0, 0), (1, 1)]
    @pl.when(core == 0)
    def _():
        send_piece(0)
        send_piece(1)

    for way, which in kv_parts(1):
        kv_copy(way, 1, which).start()
    d1_parts(0)
    for j in range(1, NXC):
        q_copy(j).start()

    def d1_copy(k):
        return remote(
            dsend.at[pl.ds(((z + k) % NZ) * NXC, NXC)],
            dmid.at[pl.ds(z * NXC, NXC)],
            d1_ss.at[k],
            d1_rs.at[k],
            z_peer(k),
            t,
        )

    def d2_copy(k, j):
        zs = (z + NZ - k) % NZ
        return remote(
            dmid.at[zs * NXC + (xc + j) % NXC],
            dout.at[zs * NXC + xc],
            d2_ss.at[0],
            d2_rs.at[j if k in NEAR else NXC + j],
            xc_peer(j),
            t,
        )

    def o1_copy(h, k):
        return remote(
            osend.at[h, pl.ds(((z + k) % NZ) * NXC, NXC)],
            omid.at[h, pl.ds(z * NXC, NXC)],
            o1_ss.at[h * NZ + k],
            o1_rs.at[h * NZ + k],
            z_peer(k),
            t,
        )

    def o2_copy(h, k, j):
        zs = (z + NZ - k) % NZ
        return remote(
            omid.at[h, zs * NXC + (xc + j) % NXC],
            oret.at[h, zs * NXC + xc],
            o2_ss.at[h],
            o2_rs.at[h * NXC + j],
            xc_peer(j),
            t,
        )

    def d2_whole(j, count, far=0):
        return remote(
            dmid.at[pl.ds(0, count)],
            dout.at[pl.ds(0, count)],
            d2_ss.at[0],
            d2_rs.at[far * NXC + j],
            xc_peer(j),
            t,
        )

    def o2_whole(h, j, count):
        return remote(
            omid.at[h, pl.ds(0, count)],
            oret.at[h, pl.ds(0, count)],
            o2_ss.at[h],
            o2_rs.at[h * NXC + j],
            xc_peer(j),
            t,
        )

    def d2_stage(k):
        if k:
            d1_copy(k).wait_recv()

        @pl.loop(1, NXC)
        def _(j):
            d2_copy(k, j).start()

        zs = (z + NZ - k) % NZ
        dout[zs * NXC + xc] = dmid[zs * NXC + xc]

    dmid[pl.ds(z * NXC, NXC)] = dsend[pl.ds(z * NXC, NXC)]

    for step in range(1, 5):
        for way, which in kv_parts(step):
            kv_copy(way, step, which).wait_recv()
        if step < 4:
            for way, which in kv_parts(step + 1):
                kv_copy(way, step + 1, which).start()
        if step < 4:
            d1_parts(step)
        if step == 2:

            @pl.when(core == 0)
            def _():
                forward_piece(0)

        if step == 3:
            for k in Z_ORDER[2:]:
                d1_copy(k).start()
    @pl.when(core == 0)
    def _():
        forward_piece(1)
        for h in range(NCH):
            send_piece(2 + h)

    for load in loads[1:4]:
        load.wait()
    for j in range(1, NXC):
        q_copy(j).wait_recv()

    lane = lax.broadcasted_iota(jnp.int32, (ROWS, 128), 1)

    def p_copy(j):
        return remote(
            psend.at[(xc + j) % NXC], precv.at[xc], p_ss.at[j], p_rs.at[j], xc_peer(j), t
        )

    def attend(j, dst):
        source = (xc + j) % NXC
        stats = jnp.zeros((ROWS, 128), F32)
        for h in range(2):
            cols = pl.ds(h * 128, 128)
            query = qbuf[source, :, cols].astype(F32) * 0.125
            keys = kbuf[:, :, cols].reshape(NZ * ROWS, 128)
            values = vbuf[:, :, cols].reshape(NZ * ROWS, 128)
            for m in range(2):
                own = (lane >= 64) if m else (lane < 64)
                masked = jnp.where(own, query, 0.0).astype(BF16)
                scores = lax.dot_general(
                    masked, keys, (((1,), (1,)), ((), ())), preferred_element_type=F32
                )
                top = jnp.max(scores, axis=1, keepdims=True)
                weights = jnp.exp(scores - top)
                total = jnp.sum(weights, axis=1, keepdims=True)
                summed = dot(weights.astype(BF16), values)
                i = h * 2 + m
                dst[:, pl.ds(i * 128, 128)] = (summed / total).astype(BF16)
                lse = top + jnp.log(total)
                high = lse.astype(BF16).astype(F32)
                mid = (lse - high).astype(BF16).astype(F32)
                low = lse - high - mid
                stats = jnp.where(lane == i, high, stats)
                stats = jnp.where(lane == 4 + i, mid, stats)
                stats = jnp.where(lane == 8 + i, low, stats)
        dst[:, pl.ds(512, 128)] = stats.astype(BF16)

    def attend_range(first, last, sent):
        @pl.loop(first, last)
        def _(j):
            attend(j, psend.at[(xc + j) % NXC])
            if sent:
                p_copy(j).start()
    attend_range(1, 3, True)
    for k in (0, 1, 7):
        d2_stage(k)
    attend_range(3, 6, True)
    d2_stage(2)
    d2_stage(6)
    attend_range(6, NXC, False)
    attend(0, precv.at[xc])

    @pl.when(core == 1)
    def _():
        send_piece(0)
        send_piece(1)
        send_piece(2)
    @pl.when(core == 0)
    def _():
        for h in range(NCH // 2):
            forward_piece(2 + h)
    d2_stage(3)
    d2_stage(5)
    @pl.when(core == 0)
    def _():
        for h in range(NCH // 2, NCH):
            forward_piece(2 + h)
    d2_stage(4)

    for j in range(6, NXC):
        p_copy(j).start()

    def a_copy(y):
        return remote(
            att.at[(t + y) % NT], attall.at[t], a_ss.at[y], a_rs.at[y], ep, (t + y) % NT
        )

    def merge():
        for j in range(1, NXC):
            p_copy(j).wait_recv()
        lses = []
        for d in range(NXC):
            stats = precv[d, :, pl.ds(512, 128)].astype(F32)
            lses.append(stats + pltpu.roll(stats, 124, 1) + pltpu.roll(stats, 120, 1))
        highest = lses[0]
        for d in range(1, NXC):
            highest = jnp.maximum(highest, lses[d])
        shares = [jnp.exp(lses[d] - highest) for d in range(NXC)]
        whole = shares[0]
        for d in range(1, NXC):
            whole = whole + shares[d]
        for d in range(NXC):
            shares[d] = shares[d] / whole
        for h in range(2):
            mixed = []
            for m in range(2):
                i = h * 2 + m
                acc = jnp.zeros((ROWS, 128), F32)
                for d in range(NXC):
                    acc = acc + shares[d][:, i : i + 1] * precv[d, :, pl.ds(i * 128, 128)].astype(F32)
                mixed.append(acc)
            per_head = mixed[0] - lam_ref[h] * mixed[1]
            squared = jnp.mean(per_head * per_head, axis=1, keepdims=True)
            normed = per_head * lax.rsqrt(squared + EPS) * hg_ref[...] * HEAD_SCALE
            for y in range(NT):
                att[y, :, pl.ds(h * 128, 128)] = normed[y * 48 : (y + 1) * 48].astype(BF16)

        for y in range(1, NT):
            a_copy(y).start()
        attall[t] = att[t]
    @pl.when(core == 1)
    def _():
        forward_piece(0)
        forward_piece(1)
        forward_piece(2)
        send_piece(3)
        send_piece(4)

    for load in loads[4:6]:
        load.wait()

    def take_rows(far):
        first, last = (5, NZ) if far else (0, 5)
        for j in range(1, NXC):
            d2_whole(j, last - first, far).wait_recv()
        for i in range(first, last):
            zs = (z + NZ - ROW_ORDER[i]) % NZ
            xall[pl.ds(i * ZROWS, ZROWS), :] = dout[pl.ds(zs * NXC, NXC)].reshape(ZROWS, D)

    def hidden_block(far, off):
        rows = pl.ds(5 * ZROWS, 3 * ZROWS) if far else pl.ds(0, 5 * ZROWS)
        b = (t + off) % NT
        arrived = xall[rows, :]
        gate_part = dot(arrived, wgb[b])
        up_part = dot(arrived, wub[b])
        hidden = gate_part / (1.0 + jnp.exp(-gate_part)) * up_part
        hid[rows, pl.ds(pl.multiple_of(b * UNITS, UNITS), UNITS)] = hidden.astype(BF16)

    def opposite_weights():
        for piece in range(2):
            for way in range(2):
                w_forward(way, piece).wait_recv()
    take_rows(0)
    for off in (0, 1, 3):
        hidden_block(0, off)

    @pl.when(core == 0)
    def _():
        opposite_weights()
        hidden_block(0, 2)
    take_rows(1)
    for off in (0, 1, 3):
        hidden_block(1, off)
    @pl.when(core == 1)
    def _():
        merge()
    @pl.when(core == 1)
    def _():
        opposite_weights()
        hidden_block(0, 2)
    hidden_block(1, 2)
    @pl.when(core == 1)
    def _():
        forward_piece(3)
        send_piece(5)

    def down(h):
        loads[7 + h].wait()
        for way in range(2):
            w_forward(way, 2 + h).wait_recv()

        for r in range(2):
            result = dot(hid[pl.ds(r * 256, 256), :], wdb[h].reshape(NT * UNITS, CW))
            for i in range(4):
                zs = (z + NZ - ROW_ORDER[r * 4 + i]) % NZ
                block = result[i * ZROWS : (i + 1) * ZROWS].reshape(NXC, CAP, CW)
                osend[h, pl.ds(zs * NXC, NXC)] = block.astype(BF16)

        for k in Z_ORDER:
            o1_copy(h, k).start()
        omid[h, pl.ds(z * NXC, NXC)] = osend[h, pl.ds(z * NXC, NXC)]

    def o2_stage(h, k):
        if k:
            o1_copy(h, k).wait_recv()

        @pl.loop(1, NXC)
        def _(j):
            o2_copy(h, k, j).start()

        zs = (z + NZ - k) % NZ
        oret[h, zs * NXC + xc] = omid[h, zs * NXC + xc]

    def o2_stages(h):
        for k in (0,) + Z_ORDER:
            o2_stage(h, k)

    def combine(h):
        for j in range(1, NXC):
            o2_whole(h, j, NZ).wait_recv()

        result = dot(gmat[...], oret[h].reshape(SLOTS, CW))
        moe_ref[:, pl.ds(h * CW, CW)] = (result[:TOK] + result[TOK:]).astype(BF16)

    def project():
        loads[6].wait()
        for y in range(1, NT):
            a_copy(y).wait_recv()
        for c in range(4):
            cols = pl.ds(c * 512, 512)
            acc = dot(attall[0], wob[pl.ds(0, 256), cols])
            for y in range(1, NT):
                acc = acc + dot(attall[y], wob[pl.ds(y * 256, 256), cols])
            mix_ref[:, cols] = acc.astype(BF16)
    @pl.when(core == 0)
    def _():
        for h in range(NCH):
            down(h)
        merge()
        for h in range(NCH):
            o2_stages(h)
        project()
    @pl.when(core == 1)
    def _():
        for h in range(NCH):
            down(h)
            if h + 2 < NCH:
                forward_piece(2 + h + 2)
            if h + 4 < NCH:
                send_piece(2 + h + 4)
            if h >= 3:
                o2_stages(h - 3)
            if h == 4:
                project()
        o2_stages(NCH - 3)
        o2_stages(NCH - 2)
    for h in range(NCH - 2):
        combine(h)
    @pl.when(core == 1)
    def _():
        o2_stages(NCH - 1)
    combine(NCH - 2)
    combine(NCH - 1)
    for j in range(1, NXC):
        q_copy(j).wait_send()
        p_copy(j).wait_send()
    for step in range(1, 5):
        for way, which in kv_parts(step):
            kv_copy(way, step, which).wait_send()
    for k in range(1, NZ):
        d1_copy(k).wait_send()
        for h in range(NCH):
            o1_copy(h, k).wait_send()
    for y in range(1, NT):
        a_copy(y).wait_send()
    for way in range(2):
        for piece in range(2 + NCH):
            w_own(way, piece).wait_send()
            w_forward(way, piece).wait_send()

    d2_whole(1, 56).wait_send()
    for h in range(NCH):
        o2_whole(h, 1, 56).wait_send()


def local(
    query_rows,
    key_rows,
    value_rows,
    lambdas,
    head_gain,
    w_out,
    moe_rows,
    ffn_gain,
    routes,
    group_logits,
    pick_logits,
    w_gate,
    w_up,
    w_down,
):
    any_ = pl.BlockSpec(memory_space=pl.ANY)
    vmem = pl.BlockSpec(memory_space=pltpu.VMEM)
    smem = pl.BlockSpec(memory_space=pltpu.SMEM)
    dma = pltpu.SemaphoreType.DMA
    return pl.pallas_call(
        kernel,
        out_shape=(
            jax.ShapeDtypeStruct((ROWS // NT, D), BF16),
            jax.ShapeDtypeStruct((TOK, D), BF16),
        ),
        in_specs=[any_, any_, any_, smem, vmem, any_, any_, vmem, vmem, vmem, vmem, any_, any_, any_],
        out_specs=(vmem, vmem),
        scratch_shapes=[
            pltpu.VMEM((NXC, ROWS, 256), BF16),
            pltpu.VMEM((NZ, ROWS, 256), BF16),
            pltpu.VMEM((NZ, ROWS, 256), BF16),
            pltpu.VMEM((NXC, ROWS, 640), BF16),
            pltpu.VMEM((NXC, ROWS, 640), BF16),
            pltpu.VMEM((NT, 48, 256), BF16),
            pltpu.VMEM((NT, 48, 256), BF16),
            pltpu.VMEM((1024, D), BF16),
            pltpu.VMEM((TOK, D), BF16),
            pltpu.VMEM((2 * TOK, SLOTS), BF16),
            pltpu.VMEM((EXPERTS, CAP, D), BF16),
            pltpu.VMEM((EXPERTS, CAP, D), BF16),
            pltpu.VMEM((EXPERTS, CAP, D), BF16),
            pltpu.VMEM((SLOTS, D), BF16),
            pltpu.VMEM((NT, D, UNITS), BF16),
            pltpu.VMEM((NT, D, UNITS), BF16),
            pltpu.VMEM((NCH, NT, UNITS, CW), BF16),
            pltpu.VMEM((SLOTS, 1024), BF16),
            pltpu.VMEM((NCH, EXPERTS, CAP, CW), BF16),
            pltpu.VMEM((NCH, EXPERTS, CAP, CW), BF16),
            pltpu.VMEM((NCH, EXPERTS, CAP, CW), BF16),
            dma((15,)),
            dma((NXC,)),
            dma((NXC,)),
            dma((20,)),
            dma((20,)),
            dma((NXC,)),
            dma((NXC,)),
            dma((NT,)),
            dma((NT,)),
            dma((2 * (2 + NCH),)),
            dma((2 * (2 + NCH),)),
            dma((2 * (2 + NCH),)),
            dma((2 * (2 + NCH),)),
            dma((NZ,)),
            dma((NZ,)),
            dma((1,)),
            dma((2 * NXC,)),
            dma((NCH * NZ,)),
            dma((NCH * NZ,)),
            dma((NCH,)),
            dma((NCH * NXC,)),
        ],
        compiler_params=pltpu.CompilerParams(
            collective_id=0, has_side_effects=True, vmem_limit_bytes=66_000_000
        ),
    )(
        query_rows,
        key_rows,
        value_rows,
        lambdas,
        head_gain[None],
        w_out,
        moe_rows,
        ffn_gain[None],
        routes.T,
        group_logits.T,
        pick_logits.T,
        w_gate,
        w_up,
        w_down,
    )


def solution(mesh):
    return jax.shard_map(
        local,
        mesh=mesh,
        in_specs=(
            P("ep", "tp"),
            P("ep", "tp"),
            P("ep", "tp"),
            P("tp"),
            P(),
            P(),
            P("ep", None),
            P(),
            P("ep", None),
            P("ep", None),
            P("ep", None),
            P("ep", None, "tp"),
            P("ep", None, "tp"),
            P("ep", "tp", None),
        ),
        out_specs=(P(("ep", "tp"), None), P(("ep", "tp"), None)),
        check_vma=False,
    )
```

```python
import jax
import jax.numpy as jnp
from jax import lax
from jax.experimental import pallas as pl
from jax.experimental.pallas import tpu as pltpu
from jax.sharding import PartitionSpec as P

EPS = 1e-06
HEAD_SCALE = 0.8
NZ, NXC, NT = 8, 8, 4
CAP = 8
EXPERTS = 64
ROWS = 192
TOK = 128
D = 2048
HALF = D // 2
NCH = 8
CW = D // NCH
UNITS = 256
SLOTS = EXPERTS * CAP
Z_ORDER = (1, 7, 2, 6, 3, 5, 4)
ROW_ORDER = (0,) + Z_ORDER
NEAR = ROW_ORDER[:5]
ZROWS = NXC * CAP
F32 = jnp.float32
BF16 = jnp.bfloat16
MESH = pl.DeviceIdType.MESH


def dot(a, b):
    return lax.dot_general(a, b, (((1,), (0,)), ((), ())), preferred_element_type=F32)


def kernel(
    q_hbm,
    k_hbm,
    v_hbm,
    lam_ref,
    hg_ref,
    wo_hbm,
    moe_hbm,
    fg_ref,
    routes_ref,
    gl_ref,
    pk_ref,
    wg_hbm,
    wu_hbm,
    wd_hbm,
    mix_ref,
    moe_ref,
    qbuf,
    kbuf,
    vbuf,
    psend,
    precv,
    att,
    attall,
    wob,
    xin,
    gmat,
    dsend,
    dmid,
    dout,
    xall,
    wgb,
    wub,
    wdb,
    hid,
    osend,
    omid,
    oret,
    loc_sem,
    q_ss,
    q_rs,
    kv_ss,
    kv_rs,
    p_ss,
    p_rs,
    a_ss,
    a_rs,
    w_ss,
    w_rs,
    f_ss,
    f_rs,
    d1_ss,
    d1_rs,
    d2_ss,
    d2_rs,
    o1_ss,
    o1_rs,
    o2_ss,
    o2_rs,
):
    ep = lax.axis_index("ep")
    t = lax.axis_index("tp")
    z = ep // NXC
    xc = ep % NXC
    core = ep % 2

    def z_peer(k):
        return ((z + k) % NZ) * NXC + xc

    def xc_peer(j):
        return z * NXC + (xc + j) % NXC

    def remote(src, dst, ssem, rsem, to_ep, to_tp):
        return pltpu.make_async_remote_copy(
            src_ref=src,
            dst_ref=dst,
            send_sem=ssem,
            recv_sem=rsem,
            device_id=(to_ep, to_tp),
            device_id_type=MESH,
        )
    base = pl.multiple_of(t * TOK, TOK)
    locals_ = [
        (moe_hbm.at[pl.ds(base, TOK)], xin),
        (q_hbm, qbuf.at[xc]),
        (k_hbm, kbuf.at[z]),
        (v_hbm, vbuf.at[z]),
        (wg_hbm.at[0], wgb.at[t]),
        (wu_hbm.at[0], wub.at[t]),
        (wo_hbm, wob),
    ] + [(wd_hbm.at[0, :, pl.ds(h * CW, CW)], wdb.at[h, t]) for h in range(NCH)]
    loads = [
        pltpu.make_async_copy(src, dst, loc_sem.at[i]) for i, (src, dst) in enumerate(locals_)
    ]
    for load in loads:
        load.start()

    barrier = pltpu.get_barrier_semaphore()
    for k in range(1, NZ):
        pl.semaphore_signal(barrier, inc=1, device_id=(z_peer(k), t), device_id_type=MESH)
    for j in range(1, NXC):
        pl.semaphore_signal(barrier, inc=1, device_id=(xc_peer(j), t), device_id_type=MESH)
    for y in range(1, NT):
        pl.semaphore_signal(barrier, inc=1, device_id=(ep, (t + y) % NT), device_id_type=MESH)
    mine = pl.ds(base, TOK)
    pick0 = routes_ref[0:1, mine]
    pick1 = routes_ref[1:2, mine]
    expert_iota = lax.broadcasted_iota(jnp.int32, (EXPERTS, TOK), 0)
    one0 = (pick0 == expert_iota).astype(F32)
    one1 = (pick1 == expert_iota).astype(F32)
    earlier = (
        lax.broadcasted_iota(jnp.int32, (TOK, TOK), 0)
        < lax.broadcasted_iota(jnp.int32, (TOK, TOK), 1)
    ).astype(BF16)
    before0 = dot(one0.astype(BF16), earlier)
    before1 = dot(one1.astype(BF16), earlier) + jnp.sum(one0, axis=1, keepdims=True)
    rank0 = jnp.sum(before0 * one0, axis=0, keepdims=True)
    rank1 = jnp.sum(before1 * one1, axis=0, keepdims=True)
    slot_iota = lax.broadcasted_iota(jnp.int32, (SLOTS, TOK), 0)
    hit0 = slot_iota == pick0 * CAP + rank0.astype(jnp.int32)
    hit1 = slot_iota == pick1 * CAP + rank1.astype(jnp.int32)

    spread = (hit0 | hit1).astype(F32).astype(BF16)
    loads[0].wait()
    rows = xin[...].astype(F32)
    squared = jnp.mean(rows * rows, axis=1, keepdims=True)
    xin[...] = (rows * lax.rsqrt(squared + EPS) * fg_ref[...]).astype(BF16)
    for c in range(4):
        cols = pl.ds(c * 512, 512)
        laid = dot(spread, xin[:, cols])
        dsend[:, :, cols] = laid.reshape(EXPERTS, CAP, 512).astype(BF16)

    groups = gl_ref[:, mine]
    group_exp = jnp.exp(groups - jnp.max(groups, axis=0, keepdims=True))
    group_prob = group_exp / jnp.sum(group_exp, axis=0, keepdims=True)
    group_iota = lax.broadcasted_iota(jnp.int32, (4, TOK), 0)
    share0 = jnp.sum(jnp.where((pick0 >> 4) == group_iota, group_prob, 0.0), axis=0, keepdims=True)
    share1 = jnp.sum(jnp.where((pick1 >> 4) == group_iota, group_prob, 0.0), axis=0, keepdims=True)
    pick_logits = pk_ref[:, mine]
    pick_exp = jnp.exp(pick_logits - jnp.max(pick_logits, axis=0, keepdims=True))
    pick_prob = pick_exp / jnp.sum(pick_exp, axis=0, keepdims=True)
    gate0 = share0 * pick_prob[0:1]
    gate1 = share1 * pick_prob[1:2]
    gates = (jnp.where(hit0, gate0, 0.0) + jnp.where(hit1, gate1, 0.0)).T
    gates_high = gates.astype(BF16)
    gmat[pl.ds(0, TOK), :] = gates_high
    gmat[pl.ds(TOK, TOK), :] = (gates - gates_high.astype(F32)).astype(BF16)
    pl.semaphore_wait(barrier, NZ - 1 + NXC - 1 + NT - 1)

    right = (t + 1) % NT
    left = (t + 3) % NT

    def w_piece(owner, piece, half=None):
        if piece < 2:
            buf = wgb if piece == 0 else wub
            if half is None:
                return buf.at[owner]
            return buf.at[owner, pl.ds(half * HALF, HALF)]
        if half is None:
            return wdb.at[piece - 2, owner]
        return wdb.at[piece - 2, owner, pl.ds(half * (UNITS // 2), UNITS // 2)]

    def w_source(piece):
        if piece == 0:
            return wg_hbm.at[0]
        if piece == 1:
            return wu_hbm.at[0]
        return wd_hbm.at[0, :, pl.ds((piece - 2) * CW, CW)]

    def w_own(way, piece):
        to = right if way == 0 else left
        return remote(
            w_source(piece),
            w_piece(t, piece),
            w_ss.at[way * (2 + NCH) + piece],
            w_rs.at[way * (2 + NCH) + piece],
            ep,
            to,
        )

    def w_forward(way, piece):
        owner = left if way == 0 else right
        to = right if way == 0 else left
        return remote(
            w_piece(owner, piece, way),
            w_piece(owner, piece, way),
            f_ss.at[way * (2 + NCH) + piece],
            f_rs.at[way * (2 + NCH) + piece],
            ep,
            to,
        )

    def send_piece(piece):
        for way in range(2):
            w_own(way, piece).start()

    def forward_piece(piece):
        for way in range(2):
            w_own(way, piece).wait_recv()
            w_forward(way, piece).start()

    def q_copy(j):
        return remote(q_hbm, qbuf.at[xc], q_ss.at[j], q_rs.at[j], xc_peer(j), t)

    def kv_copy(way, step, which):
        shift = 1 - step if way == 0 else step - 1
        slot = (z + NZ + shift) % NZ
        buf = vbuf if which else kbuf
        src = (v_hbm if which else k_hbm) if step == 1 else buf.at[slot]
        i = (way * 5 + step) * 2 + which
        return remote(
            src, buf.at[slot], kv_ss.at[i], kv_rs.at[i], z_peer(1 if way == 0 else NZ - 1), t
        )

    def d1_part(k, part):
        return remote(
            dsend.at[pl.ds(((z + k) % NZ) * NXC + part * 2, 2)],
            dmid.at[pl.ds(z * NXC + part * 2, 2)],
            d1_ss.at[k],
            d1_rs.at[k],
            z_peer(k),
            t,
        )

    def d1_parts(part):
        d1_part(1, part).start()
        d1_part(7, part).start()

    def kv_parts(step):
        if step < 4:
            return [(0, 0), (0, 1), (1, 0), (1, 1)]
        return [(0, 0), (1, 1)]
    @pl.when(core == 0)
    def _():
        send_piece(0)
        send_piece(1)

    for way, which in kv_parts(1):
        kv_copy(way, 1, which).start()
    d1_parts(0)
    for j in range(1, NXC):
        q_copy(j).start()

    def d1_copy(k):
        return remote(
            dsend.at[pl.ds(((z + k) % NZ) * NXC, NXC)],
            dmid.at[pl.ds(z * NXC, NXC)],
            d1_ss.at[k],
            d1_rs.at[k],
            z_peer(k),
            t,
        )

    def d2_copy(k, j):
        zs = (z + NZ - k) % NZ
        return remote(
            dmid.at[zs * NXC + (xc + j) % NXC],
            dout.at[zs * NXC + xc],
            d2_ss.at[0],
            d2_rs.at[j if k in NEAR else NXC + j],
            xc_peer(j),
            t,
        )

    def o1_copy(h, k):
        return remote(
            osend.at[h, pl.ds(((z + k) % NZ) * NXC, NXC)],
            omid.at[h, pl.ds(z * NXC, NXC)],
            o1_ss.at[h * NZ + k],
            o1_rs.at[h * NZ + k],
            z_peer(k),
            t,
        )

    def o2_copy(h, k, j):
        zs = (z + NZ - k) % NZ
        return remote(
            omid.at[h, zs * NXC + (xc + j) % NXC],
            oret.at[h, zs * NXC + xc],
            o2_ss.at[h],
            o2_rs.at[h * NXC + j],
            xc_peer(j),
            t,
        )

    def d2_whole(j, count, far=0):
        return remote(
            dmid.at[pl.ds(0, count)],
            dout.at[pl.ds(0, count)],
            d2_ss.at[0],
            d2_rs.at[far * NXC + j],
            xc_peer(j),
            t,
        )

    def o2_whole(h, j, count):
        return remote(
            omid.at[h, pl.ds(0, count)],
            oret.at[h, pl.ds(0, count)],
            o2_ss.at[h],
            o2_rs.at[h * NXC + j],
            xc_peer(j),
            t,
        )

    def d2_stage(k):
        if k:
            d1_copy(k).wait_recv()

        @pl.loop(1, NXC)
        def _(j):
            d2_copy(k, j).start()

        zs = (z + NZ - k) % NZ
        dout[zs * NXC + xc] = dmid[zs * NXC + xc]

    dmid[pl.ds(z * NXC, NXC)] = dsend[pl.ds(z * NXC, NXC)]

    for step in range(1, 5):
        for way, which in kv_parts(step):
            kv_copy(way, step, which).wait_recv()
        if step < 4:
            for way, which in kv_parts(step + 1):
                kv_copy(way, step + 1, which).start()
        if step < 4:
            d1_parts(step)
        if step == 2:

            @pl.when(core == 0)
            def _():
                forward_piece(0)

        if step == 3:
            for k in Z_ORDER[2:]:
                d1_copy(k).start()
    @pl.when(core == 0)
    def _():
        forward_piece(1)
        for h in range(NCH):
            send_piece(2 + h)

    for load in loads[1:4]:
        load.wait()
    for j in range(1, NXC):
        q_copy(j).wait_recv()

    lane = lax.broadcasted_iota(jnp.int32, (ROWS, 128), 1)

    def p_copy(j):
        return remote(
            psend.at[(xc + j) % NXC], precv.at[xc], p_ss.at[j], p_rs.at[j], xc_peer(j), t
        )

    def attend(j, dst):
        source = (xc + j) % NXC
        stats = jnp.zeros((ROWS, 128), F32)
        for h in range(2):
            cols = pl.ds(h * 128, 128)
            query = qbuf[source, :, cols].astype(F32) * 0.125
            keys = kbuf[:, :, cols].reshape(NZ * ROWS, 128)
            values = vbuf[:, :, cols].reshape(NZ * ROWS, 128)
            for m in range(2):
                own = (lane >= 64) if m else (lane < 64)
                masked = jnp.where(own, query, 0.0).astype(BF16)
                scores = lax.dot_general(
                    masked, keys, (((1,), (1,)), ((), ())), preferred_element_type=F32
                )
                top = jnp.max(scores, axis=1, keepdims=True)
                weights = jnp.exp(scores - top)
                total = jnp.sum(weights, axis=1, keepdims=True)
                summed = dot(weights.astype(BF16), values)
                i = h * 2 + m
                dst[:, pl.ds(i * 128, 128)] = (summed / total).astype(BF16)
                lse = top + jnp.log(total)
                high = lse.astype(BF16).astype(F32)
                mid = (lse - high).astype(BF16).astype(F32)
                low = lse - high - mid
                stats = jnp.where(lane == i, high, stats)
                stats = jnp.where(lane == 4 + i, mid, stats)
                stats = jnp.where(lane == 8 + i, low, stats)
        dst[:, pl.ds(512, 128)] = stats.astype(BF16)

    def attend_range(first, last, sent):
        @pl.loop(first, last)
        def _(j):
            attend(j, psend.at[(xc + j) % NXC])
            if sent:
                p_copy(j).start()
    attend_range(1, 3, True)
    for k in (0, 1, 7):
        d2_stage(k)
    attend_range(3, 6, True)
    d2_stage(2)
    d2_stage(6)
    attend_range(6, NXC, False)
    attend(0, precv.at[xc])

    @pl.when(core == 1)
    def _():
        send_piece(0)
        send_piece(1)
        send_piece(2)
    @pl.when(core == 0)
    def _():
        for h in range(NCH // 2):
            forward_piece(2 + h)
    d2_stage(3)
    d2_stage(5)
    @pl.when(core == 0)
    def _():
        for h in range(NCH // 2, NCH):
            forward_piece(2 + h)
    d2_stage(4)

    for j in range(6, NXC):
        p_copy(j).start()

    def a_copy(y):
        return remote(
            att.at[(t + y) % NT], attall.at[t], a_ss.at[y], a_rs.at[y], ep, (t + y) % NT
        )

    def merge():
        for j in range(1, NXC):
            p_copy(j).wait_recv()
        lses = []
        for d in range(NXC):
            stats = precv[d, :, pl.ds(512, 128)].astype(F32)
            lses.append(stats + pltpu.roll(stats, 124, 1) + pltpu.roll(stats, 120, 1))
        highest = lses[0]
        for d in range(1, NXC):
            highest = jnp.maximum(highest, lses[d])
        shares = [jnp.exp(lses[d] - highest) for d in range(NXC)]
        whole = shares[0]
        for d in range(1, NXC):
            whole = whole + shares[d]
        for d in range(NXC):
            shares[d] = shares[d] / whole
        for h in range(2):
            mixed = []
            for m in range(2):
                i = h * 2 + m
                acc = jnp.zeros((ROWS, 128), F32)
                for d in range(NXC):
                    acc = acc + shares[d][:, i : i + 1] * precv[d, :, pl.ds(i * 128, 128)].astype(F32)
                mixed.append(acc)
            per_head = mixed[0] - lam_ref[h] * mixed[1]
            squared = jnp.mean(per_head * per_head, axis=1, keepdims=True)
            normed = per_head * lax.rsqrt(squared + EPS) * hg_ref[...] * HEAD_SCALE
            for y in range(NT):
                att[y, :, pl.ds(h * 128, 128)] = normed[y * 48 : (y + 1) * 48].astype(BF16)

        for y in range(1, NT):
            a_copy(y).start()
        attall[t] = att[t]
    @pl.when(core == 1)
    def _():
        forward_piece(0)
        forward_piece(1)
        forward_piece(2)
        send_piece(3)
        send_piece(4)

    for load in loads[4:6]:
        load.wait()

    def take_rows(far):
        first, last = (5, NZ) if far else (0, 5)
        for j in range(1, NXC):
            d2_whole(j, last - first, far).wait_recv()
        for i in range(first, last):
            zs = (z + NZ - ROW_ORDER[i]) % NZ
            xall[pl.ds(i * ZROWS, ZROWS), :] = dout[pl.ds(zs * NXC, NXC)].reshape(ZROWS, D)

    def hidden_block(far, off):
        rows = pl.ds(5 * ZROWS, 3 * ZROWS) if far else pl.ds(0, 5 * ZROWS)
        b = (t + off) % NT
        arrived = xall[rows, :]
        gate_part = dot(arrived, wgb[b])
        up_part = dot(arrived, wub[b])
        hidden = gate_part / (1.0 + jnp.exp(-gate_part)) * up_part
        hid[rows, pl.ds(pl.multiple_of(b * UNITS, UNITS), UNITS)] = hidden.astype(BF16)

    def opposite_weights():
        for piece in range(2):
            for way in range(2):
                w_forward(way, piece).wait_recv()

    def down(h, far):
        if not far:
            loads[7 + h].wait()
            for way in range(2):
                w_forward(way, 2 + h).wait_recv()
        first, last = (5, NZ) if far else (0, 5)
        rows = pl.ds(first * ZROWS, (last - first) * ZROWS)
        result = dot(hid[rows, :], wdb[h].reshape(NT * UNITS, CW))
        for i in range(first, last):
            zs = (z + NZ - ROW_ORDER[i]) % NZ
            block = result[(i - first) * ZROWS : (i - first + 1) * ZROWS].reshape(NXC, CAP, CW)
            osend[h, pl.ds(zs * NXC, NXC)] = block.astype(BF16)
        for k in ROW_ORDER[max(first, 1) : last]:
            o1_copy(h, k).start()
        if not far:
            omid[h, pl.ds(z * NXC, NXC)] = osend[h, pl.ds(z * NXC, NXC)]
    take_rows(0)
    for off in (0, 1, 3):
        hidden_block(0, off)

    @pl.when(core == 0)
    def _():
        opposite_weights()
        hidden_block(0, 2)
        for h in range(NCH):
            down(h, 0)
    take_rows(1)
    for off in (0, 1, 3):
        hidden_block(1, off)
    @pl.when(core == 1)
    def _():
        merge()
    @pl.when(core == 1)
    def _():
        opposite_weights()
        hidden_block(0, 2)
    hidden_block(1, 2)
    @pl.when(core == 1)
    def _():
        forward_piece(3)
        send_piece(5)

    def o2_stage(h, k):
        if k:
            o1_copy(h, k).wait_recv()

        @pl.loop(1, NXC)
        def _(j):
            o2_copy(h, k, j).start()

        zs = (z + NZ - k) % NZ
        oret[h, zs * NXC + xc] = omid[h, zs * NXC + xc]

    def o2_stages(h):
        for k in (0,) + Z_ORDER:
            o2_stage(h, k)

    def combine(h):
        for j in range(1, NXC):
            o2_whole(h, j, NZ).wait_recv()

        result = dot(gmat[...], oret[h].reshape(SLOTS, CW))
        moe_ref[:, pl.ds(h * CW, CW)] = (result[:TOK] + result[TOK:]).astype(BF16)

    def project():
        loads[6].wait()
        for y in range(1, NT):
            a_copy(y).wait_recv()
        for c in range(4):
            cols = pl.ds(c * 512, 512)
            acc = dot(attall[0], wob[pl.ds(0, 256), cols])
            for y in range(1, NT):
                acc = acc + dot(attall[y], wob[pl.ds(y * 256, 256), cols])
            mix_ref[:, cols] = acc.astype(BF16)
    @pl.when(core == 0)
    def _():
        for h in range(NCH):
            down(h, 1)
        merge()
        for h in range(NCH):
            o2_stages(h)
        project()
    @pl.when(core == 1)
    def _():
        for h in range(NCH):
            down(h, 0)
            down(h, 1)
            if h + 2 < NCH:
                forward_piece(2 + h + 2)
            if h + 4 < NCH:
                send_piece(2 + h + 4)
            if h >= 3:
                o2_stages(h - 3)
            if h == 4:
                project()
        o2_stages(NCH - 3)
        o2_stages(NCH - 2)
    for h in range(NCH - 2):
        combine(h)
    @pl.when(core == 1)
    def _():
        o2_stages(NCH - 1)
    combine(NCH - 2)
    combine(NCH - 1)
    for j in range(1, NXC):
        q_copy(j).wait_send()
        p_copy(j).wait_send()
    for step in range(1, 5):
        for way, which in kv_parts(step):
            kv_copy(way, step, which).wait_send()
    for k in range(1, NZ):
        d1_copy(k).wait_send()
        for h in range(NCH):
            o1_copy(h, k).wait_send()
    for y in range(1, NT):
        a_copy(y).wait_send()
    for way in range(2):
        for piece in range(2 + NCH):
            w_own(way, piece).wait_send()
            w_forward(way, piece).wait_send()

    d2_whole(1, 56).wait_send()
    for h in range(NCH):
        o2_whole(h, 1, 56).wait_send()


def local(
    query_rows,
    key_rows,
    value_rows,
    lambdas,
    head_gain,
    w_out,
    moe_rows,
    ffn_gain,
    routes,
    group_logits,
    pick_logits,
    w_gate,
    w_up,
    w_down,
):
    any_ = pl.BlockSpec(memory_space=pl.ANY)
    vmem = pl.BlockSpec(memory_space=pltpu.VMEM)
    smem = pl.BlockSpec(memory_space=pltpu.SMEM)
    dma = pltpu.SemaphoreType.DMA
    return pl.pallas_call(
        kernel,
        out_shape=(
            jax.ShapeDtypeStruct((ROWS // NT, D), BF16),
            jax.ShapeDtypeStruct((TOK, D), BF16),
        ),
        in_specs=[any_, any_, any_, smem, vmem, any_, any_, vmem, vmem, vmem, vmem, any_, any_, any_],
        out_specs=(vmem, vmem),
        scratch_shapes=[
            pltpu.VMEM((NXC, ROWS, 256), BF16),
            pltpu.VMEM((NZ, ROWS, 256), BF16),
            pltpu.VMEM((NZ, ROWS, 256), BF16),
            pltpu.VMEM((NXC, ROWS, 640), BF16),
            pltpu.VMEM((NXC, ROWS, 640), BF16),
            pltpu.VMEM((NT, 48, 256), BF16),
            pltpu.VMEM((NT, 48, 256), BF16),
            pltpu.VMEM((1024, D), BF16),
            pltpu.VMEM((TOK, D), BF16),
            pltpu.VMEM((2 * TOK, SLOTS), BF16),
            pltpu.VMEM((EXPERTS, CAP, D), BF16),
            pltpu.VMEM((EXPERTS, CAP, D), BF16),
            pltpu.VMEM((EXPERTS, CAP, D), BF16),
            pltpu.VMEM((SLOTS, D), BF16),
            pltpu.VMEM((NT, D, UNITS), BF16),
            pltpu.VMEM((NT, D, UNITS), BF16),
            pltpu.VMEM((NCH, NT, UNITS, CW), BF16),
            pltpu.VMEM((SLOTS, 1024), BF16),
            pltpu.VMEM((NCH, EXPERTS, CAP, CW), BF16),
            pltpu.VMEM((NCH, EXPERTS, CAP, CW), BF16),
            pltpu.VMEM((NCH, EXPERTS, CAP, CW), BF16),
            dma((15,)),
            dma((NXC,)),
            dma((NXC,)),
            dma((20,)),
            dma((20,)),
            dma((NXC,)),
            dma((NXC,)),
            dma((NT,)),
            dma((NT,)),
            dma((2 * (2 + NCH),)),
            dma((2 * (2 + NCH),)),
            dma((2 * (2 + NCH),)),
            dma((2 * (2 + NCH),)),
            dma((NZ,)),
            dma((NZ,)),
            dma((1,)),
            dma((2 * NXC,)),
            dma((NCH * NZ,)),
            dma((NCH * NZ,)),
            dma((NCH,)),
            dma((NCH * NXC,)),
        ],
        compiler_params=pltpu.CompilerParams(
            collective_id=0, has_side_effects=True, vmem_limit_bytes=66_000_000
        ),
    )(
        query_rows,
        key_rows,
        value_rows,
        lambdas,
        head_gain[None],
        w_out,
        moe_rows,
        ffn_gain[None],
        routes.T,
        group_logits.T,
        pick_logits.T,
        w_gate,
        w_up,
        w_down,
    )


def solution(mesh):
    return jax.shard_map(
        local,
        mesh=mesh,
        in_specs=(
            P("ep", "tp"),
            P("ep", "tp"),
            P("ep", "tp"),
            P("tp"),
            P(),
            P(),
            P("ep", None),
            P(),
            P("ep", None),
            P("ep", None),
            P("ep", None),
            P("ep", None, "tp"),
            P("ep", None, "tp"),
            P("ep", "tp", None),
        ),
        out_specs=(P(("ep", "tp"), None), P(("ep", "tp"), None)),
        check_vma=False,
    )
```
